512 devices in a mesh: sp: 64 (over z, y), tp: 8 (over x, core).
Axes of the slice: x: 4, y: 8, z: 8, core: 2. Of those that a mesh axis runs over, the one named last changes fastest.
Arguments:
- resid: bfloat16 [8192, 2048], P(('sp', 'tp')), may hold values from -3 to 3
- queries: bfloat16 [8192, 2048], P('sp', 'tp'), may hold values from -6 to 6
- keys: bfloat16 [8192, 2048], P('sp', 'tp'), may hold values from -6 to 6
- values: bfloat16 [8192, 2048], P('sp', 'tp'), may hold values from -8 to 8
- doc_ids: int32 [8192], P('sp'), may hold values from 0 to 15, never falling along the last dimension, each value on 1 to 896 neighbouring positions
- score_offset: float32 [32], P('tp'), may hold values from -10 to -3
- out_weight: bfloat16 [2048, 2048], P('tp'), may hold values from -0.1875 to 0.1875
- norm_gain: float32 [2048], replicated, may hold values from 0.1 to 1.9
- gate_weight: bfloat16 [2048, 6144], P('sp', 'tp'), may hold values from -0.125 to 0.125
- up_weight: bfloat16 [2048, 6144], P('sp', 'tp'), may hold values from -0.125 to 0.125
- down_weight: bfloat16 [6144, 2048], P('tp', 'sp'), may hold values from -0.078125 to 0.078125
Outputs:
- layer_out: bfloat16 [8192, 2048], P(('sp', 'tp'))
The draws below stay inside these ranges and needn't reach their ends.
Inputs may be any that keep to these rules, and one draw needn't show every extreme that they name: `doc_ids`: document numbers never fall along the sequence; each document has 1 to 896 positions, and one has exactly 896.
All inputs are finite; a program needn't handle non-finite values.
Results may differ from the reference program's by a relative error of at most 0.017.
Values may be sent and summed in bfloat16 or wider, within the bound.
No kernel may reach another device: no remote copies, remote signals or barrier semaphores. Data moves between devices by JAX's collectives and lax.ppermute only.
A program may use at most 64 MiB of HBM per device.

```python
import math
import jax
import jax.numpy as jnp
import numpy as np
from jax import lax

D = 2048
HEADS = 32
HEAD_DIM = 64
FF = 6144
TOK_DEV = 128
TOKENS = 8192
DOCS = 16
DOC_MOST = 896
N_TP = 8


def draw_score_offset(key, part):
    pick_key = jax.random.fold_in(key, 11)
    slow_key = jax.random.fold_in(key, 12)
    fast_key = jax.random.fold_in(key, 13)
    quick = jax.random.bernoulli(pick_key, 0.5, (HEADS,))
    rate = jax.random.uniform(slow_key, (HEADS,), jnp.float32, 0.5, 2.5)
    slow_offset = jnp.log(rate / DOC_MOST) - 0.5
    fast_offset = jnp.log(jax.random.uniform(fast_key, (HEADS,), jnp.float32, 1.0 / 80.0, 1.0 / 30.0)) - 0.5
    return jnp.clip(jnp.where(quick, fast_offset, slow_offset), -10.0, -3.0).astype(jnp.float32)


def draw_values(key, part):
    span_key = jax.random.fold_in(key, 21)
    noise_key = jax.random.fold_in(key, 22)
    width = HEADS * HEAD_DIM
    spans = TOKENS // TOK_DEV
    common = jax.random.normal(span_key, (spans, 1, width), jnp.float32)
    noise = 0.5 * jax.random.normal(noise_key, (spans, TOK_DEV, width), jnp.float32)
    return jnp.clip(common + noise, -8.0, 8.0).reshape(TOKENS, width).astype(jnp.bfloat16)


def shard_levels(own_key, dims, split, smallest, top_value):
    def one(position, shards_of):
        draws = jax.random.uniform(jax.random.fold_in(jax.random.fold_in(own_key, 6), position), (shards_of,), jnp.float32, smallest / len(split), top_value / len(split))
        return jnp.repeat(jnp.exp(draws), dims[position] // shards_of).reshape((-1,) + (1,) * (len(dims) - position - 1))

    factor_of = one(*split[0])
    for cut in split[1:]:
        factor_of = factor_of * one(*cut)
    return factor_of


def profile(amount, total, reach, slope):
    loads = [(1 << 20) // math.isqrt(grade ** slope) + 1 for grade in range(2, amount + 1)]
    surplus, counts = total - reach - (amount - 1), [1] * (amount - 1)
    while surplus > 0:
        movable = [i for i in range(amount - 1) if counts[i] < reach]
        whole, left = sum([loads[i] for i in movable]), surplus
        for i in movable:
            addition = min(reach - counts[i], max(1, left * loads[i] // whole), surplus)
            counts[i] = counts[i] + addition
            surplus = surplus - addition
    return np.array([reach] + counts)


def uneven_parts(stream_key, number_of, total, bound, skew):
    if number_of == 2:
        one = jax.random.randint(stream_key, (), max(1, total - bound), min(bound, total - 1) + 1)
        return jnp.stack([one, total - one])
    lengths = jnp.asarray(profile(number_of, total, bound, skew), jnp.int32)
    couples = (number_of - 1) // 2
    source_of, taker = lengths[1:1 + 2 * couples:2], lengths[2:2 + 2 * couples:2]
    margin = jnp.minimum(source_of - 1, bound - taker)
    moved = jax.random.randint(jax.random.fold_in(stream_key, 1), (couples,), 0, 1 << 20) % (margin + 1)
    lengths = lengths.at[1:1 + 2 * couples:2].set(source_of - moved).at[2:2 + 2 * couples:2].set(taker + moved)
    return lengths[jax.random.permutation(jax.random.fold_in(stream_key, 2), number_of)]


def gaussian(rng, shape, deviation, most, split=(), held_as=jnp.bfloat16):
    entries = jax.random.normal(rng, shape, jnp.float32) * deviation
    if len(split) > 0:
        entries = shard_levels(rng, shape, split, -0.22, 0.18) * entries
    return jnp.clip(entries, min=-most, max=most).astype(held_as)


def setup_inputs(seed: int = 0) -> dict:
    seeds = jax.random.split(jax.random.key(seed), 12)
    resid = gaussian(seeds[0], (TOKENS, D), 0.5, 3.0, ((0, 512),))
    queries = gaussian(seeds[1], (TOKENS, HEADS * HEAD_DIM), 1.0, 6.0, ((0, 64), (1, 8)))
    keys = gaussian(seeds[2], (TOKENS, HEADS * HEAD_DIM), 1.0, 6.0, ((0, 64), (1, 8)))
    values = draw_values(jax.random.fold_in(seeds[11], 71), 0)
    doc_ids = jnp.searchsorted(jnp.cumsum(uneven_parts(seeds[4], DOCS, TOKENS, DOC_MOST, 1)), jnp.arange(TOKENS), side="right").astype(jnp.int32)
    score_offset = draw_score_offset(jax.random.fold_in(seeds[11], 71), 0)
    out_weight = gaussian(seeds[6], (HEADS * HEAD_DIM, D), (HEADS * HEAD_DIM // 2) ** -0.5, 0.1875, ((0, 8),))
    norm_gain = jnp.clip(1.0 + 0.18 * jax.random.normal(seeds[7], (D,), jnp.float32), 0.1, 1.9)
    gate_weight = gaussian(seeds[8], (D, FF), D ** -0.5, 0.125, ((0, 64), (1, 8)))
    up_weight = gaussian(seeds[9], (D, FF), D ** -0.5, 0.125, ((0, 64), (1, 8)))
    down_weight = gaussian(seeds[10], (FF, D), FF ** -0.5, 0.078125, ((0, 8), (1, 64)))
    return dict(resid=resid, queries=queries, keys=keys, values=values, doc_ids=doc_ids, score_offset=score_offset, out_weight=out_weight, norm_gain=norm_gain, gate_weight=gate_weight, up_weight=up_weight, down_weight=down_weight)


def head_attention(q_head, k_head, v_head, doc_ids, offset):
    q_block = math.gcd(TOKENS, 512)
    extent = min(TOKENS, q_block + DOC_MOST)
    blocks = TOKENS // q_block
    scale = HEAD_DIM ** (-0.5)

    def block(index):
        start = (index * q_block).astype(jnp.int32)
        k_start = jnp.clip(start + q_block - extent, 0, TOKENS - extent).astype(jnp.int32)
        q_rows = lax.dynamic_slice_in_dim(q_head, start, q_block, 0)
        q_docs = lax.dynamic_slice_in_dim(doc_ids, start, q_block, 0)
        k_rows = lax.dynamic_slice_in_dim(k_head, k_start, extent, 0)
        v_rows = lax.dynamic_slice_in_dim(v_head, k_start, extent, 0)
        k_docs = lax.dynamic_slice_in_dim(doc_ids, k_start, extent, 0)
        q_pos = start + jnp.arange(q_block, dtype=jnp.int32)
        key_pos = k_start + jnp.arange(extent, dtype=jnp.int32)
        scores = lax.dot_general(q_rows, k_rows, (((1,), (1,)), ((), ())), preferred_element_type=jnp.float32) * scale + offset
        live = (key_pos[None, :] < q_pos[:, None]) & (k_docs[None, :] == q_docs[:, None])
        log_keep = jnp.where(live, jax.nn.log_sigmoid(-scores), 0.0)
        tail = lax.cumsum(log_keep, axis=1, reverse=True) - log_keep
        weight = jnp.where(live, jnp.exp(jax.nn.log_sigmoid(scores) + tail), 0.0).astype(jnp.bfloat16)
        return jnp.dot(weight, v_rows, preferred_element_type=jnp.float32).astype(jnp.bfloat16)
    result = lax.map(block, jnp.arange(blocks, dtype=jnp.int32))
    return result.reshape(TOKENS, HEAD_DIM)

def reference(resid, queries, keys, values, doc_ids, score_offset, out_weight, norm_gain, gate_weight, up_weight, down_weight):
    heads_out = []
    for head in range(HEADS):
        cols = slice(head * HEAD_DIM, (head + 1) * HEAD_DIM)
        heads_out.append(head_attention(queries[:, cols], keys[:, cols], values[:, cols], doc_ids, score_offset[head]))
    attended = jnp.concatenate(heads_out, axis=1)
    group_width = HEADS // N_TP * HEAD_DIM
    mixed_attn = jnp.zeros((TOKENS, D), jnp.float32)
    for group in range(N_TP):
        cols = slice(group * group_width, (group + 1) * group_width)
        partial_out = jnp.dot(attended[:, cols], out_weight[cols, :], preferred_element_type=jnp.float32)
        mixed_attn = mixed_attn + partial_out.astype(jnp.bfloat16).astype(jnp.float32)
    stream = resid.astype(jnp.float32) + mixed_attn
    normed = (stream * lax.rsqrt(lax.optimization_barrier(jnp.mean(stream * stream, axis=1, keepdims=True)) + 1e-06) * norm_gain).astype(jnp.bfloat16)
    unit_width = FF // N_TP
    feed = jnp.zeros((TOKENS, D), jnp.float32)
    for group in range(N_TP):
        cols = slice(group * unit_width, (group + 1) * unit_width)
        gate = jnp.dot(normed, gate_weight[:, cols], preferred_element_type=jnp.float32)
        upper = jnp.dot(normed, up_weight[:, cols], preferred_element_type=jnp.float32)
        hidden = (jax.nn.silu(gate) * upper).astype(jnp.bfloat16)
        partial_out = jnp.dot(hidden, down_weight[cols, :], preferred_element_type=jnp.float32)
        feed = feed + partial_out.astype(jnp.bfloat16).astype(jnp.float32)
    return (stream + feed).astype(jnp.bfloat16)
```

```python
import jax
import jax.numpy as jnp
from jax import lax
from jax.experimental import pallas as pl
from jax.experimental.pallas import tpu as pltpu
from jax.sharding import PartitionSpec as P


def shifted(block, by):
    spans = lax.axis_size("sp")
    return lax.ppermute(block, "sp", [(i, (i + by) % spans) for i in range(spans)])


def summed_for_owner(partial):
    peers = lax.axis_size("tp")
    tiles = partial.reshape(peers, partial.shape[0] // peers, partial.shape[1])
    tiles = lax.all_to_all(tiles, "tp", 0, 0, tiled=True)
    return jnp.sum(tiles.astype(jnp.float32), axis=0)


def from_everyone(shard):
    copies = jnp.broadcast_to(shard, (lax.axis_size("tp"), *shard.shape))
    return lax.all_to_all(copies, "tp", split_axis=0, concat_axis=0, tiled=True)


def attention_kernel(heads, head_dim, rows, offsets, queries, *refs):
    blocks, out = refs[:-1], refs[-1]
    width = heads * head_dim
    own_docs = blocks[0][rows : rows + 1, :rows].astype(jnp.float32)
    q_docs = jnp.broadcast_to(own_docs, (rows, rows)).T
    q_docs = jnp.concatenate([q_docs, q_docs], axis=1)
    r = lax.broadcasted_iota(jnp.int32, (rows, 2 * rows), 0)
    c = lax.broadcasted_iota(jnp.int32, (rows, 2 * rows), 1)
    causal = c - rows < r
    j = lax.broadcasted_iota(jnp.int32, (2 * rows, 2 * rows), 0)
    s = lax.broadcasted_iota(jnp.int32, (2 * rows, 2 * rows), 1)
    later = (j > s).astype(jnp.float32).astype(jnp.bfloat16)
    totals = [jnp.zeros((rows, head_dim), jnp.float32) for _ in range(heads)]
    carried = [jnp.zeros((rows, 1), jnp.float32) for _ in range(heads)]
    scale = head_dim ** (-0.5)
    for pair in range(len(blocks) // 2):
        near, far = blocks[2 * pair], blocks[2 * pair + 1]
        k_docs = jnp.concatenate([far[rows : rows + 1, :rows], near[rows : rows + 1, :rows]], axis=1)
        live = k_docs.astype(jnp.float32) == q_docs
        if pair == 0:
            live = live & causal
        for h in range(heads):
            cols = slice(h * head_dim, (h + 1) * head_dim)
            v_cols = slice(width + h * head_dim, width + (h + 1) * head_dim)
            k = jnp.concatenate([far[:rows, cols], near[:rows, cols]], axis=0)
            v = jnp.concatenate([far[:rows, v_cols], near[:rows, v_cols]], axis=0)
            z = lax.dot_general(
                queries[:, cols], k, (((1,), (1,)), ((), ())), preferred_element_type=jnp.float32
            ) * scale + offsets[h]
            soft = jnp.log(1.0 + jnp.exp(-jnp.abs(z)))
            keep = jnp.where(live, jnp.minimum(-z, 0.0) - soft, 0.0)
            high = keep.astype(jnp.bfloat16)
            low = (keep - high.astype(jnp.float32)).astype(jnp.bfloat16)
            tail = jnp.dot(high, later, preferred_element_type=jnp.float32) + jnp.dot(
                low, later, preferred_element_type=jnp.float32
            )
            weight = jnp.where(live, jnp.exp(jnp.minimum(z, 0.0) - soft + tail + carried[h]), 0.0)
            totals[h] += jnp.dot(weight.astype(jnp.bfloat16), v, preferred_element_type=jnp.float32)
            carried[h] += tail[:, :1] + keep[:, :1]
    out[...] = jnp.concatenate(totals, axis=1).astype(jnp.bfloat16)


def attention(queries, blocks, offsets):
    rows, width = queries.shape
    heads = offsets.shape[0]
    vmem = pl.BlockSpec(memory_space=pltpu.VMEM)

    def body(*refs):
        attention_kernel(heads, width // heads, rows, *refs)

    return pl.pallas_call(
        body,
        out_shape=jax.ShapeDtypeStruct((rows, width), jnp.bfloat16),
        in_specs=[pl.BlockSpec(memory_space=pltpu.SMEM)] + [vmem] * (1 + len(blocks)),
        out_specs=vmem,
        name="attention",
    )(offsets, queries, *blocks)


def on_device(
    resid,
    queries,
    keys,
    values,
    doc_ids,
    score_offset,
    out_weight,
    norm_gain,
    gate_weight,
    up_weight,
    down_weight,
):
    rows = queries.shape[0]
    units = gate_weight.shape[1]
    packed = jnp.concatenate([gate_weight, up_weight, down_weight.T], axis=1)
    weights = lax.all_gather(packed, "sp", axis=0, tiled=True)

    docs = jnp.pad(doc_ids.astype(jnp.bfloat16)[None], ((0, 15), (0, 2 * keys.shape[1] - rows)))
    own = jnp.concatenate([jnp.concatenate([keys, values], axis=1), docs], axis=0)
    blocks = {0: own}
    blocks[7] = shifted(own, 7)
    for back in range(1, 5):
        blocks[back] = shifted(blocks[back - 1], 1)
        if back < 3:
            blocks[7 - back] = shifted(blocks[8 - back], -1)
    attended = attention(queries, [blocks[b] for b in range(8)], score_offset)

    mixed_attn = summed_for_owner(
        jnp.dot(attended, out_weight, preferred_element_type=jnp.float32).astype(jnp.bfloat16)
    )
    stream = resid.astype(jnp.float32) + mixed_attn
    normed = (
        stream * lax.rsqrt(jnp.mean(stream * stream, axis=1, keepdims=True) + 1e-06) * norm_gain
    ).astype(jnp.bfloat16)
    span_rows = from_everyone(normed).reshape(rows, -1)
    gate = jnp.dot(span_rows, weights[:, :units], preferred_element_type=jnp.float32)
    upper = jnp.dot(span_rows, weights[:, units : 2 * units], preferred_element_type=jnp.float32)
    hidden = (jax.nn.silu(gate) * upper).astype(jnp.bfloat16)
    partial_out = lax.dot_general(
        hidden,
        weights[:, 2 * units :],
        (((1,), (1,)), ((), ())),
        preferred_element_type=jnp.float32,
    )
    feed = summed_for_owner(partial_out.astype(jnp.bfloat16))
    return (stream + feed).astype(jnp.bfloat16)


def solution(mesh):
    in_specs = (
        P(("sp", "tp"), None),
        P("sp", "tp"),
        P("sp", "tp"),
        P("sp", "tp"),
        P("sp"),
        P("tp"),
        P("tp", None),
        P(),
        P("sp", "tp"),
        P("sp", "tp"),
        P("tp", "sp"),
    )
    out_specs = P(("sp", "tp"), None)
    return jax.shard_map(
        on_device, mesh=mesh, in_specs=in_specs, out_specs=out_specs, check_vma=False
    )
```

```python
from functools import partial

import jax
import jax.numpy as jnp
from jax import lax
from jax.experimental import pallas as pl
from jax.experimental.pallas import tpu as pltpu
from jax.sharding import PartitionSpec as P


def shifted(block, by):
    spans = lax.axis_size("sp")
    return lax.ppermute(block, "sp", [(i, (i + by) % spans) for i in range(spans)])


def summed_for_owner(terms):
    peers = lax.axis_size("tp")
    tiles = terms.reshape(peers, terms.shape[0] // peers, terms.shape[1])
    tiles = lax.all_to_all(tiles, "tp", 0, 0, tiled=True)
    return jnp.sum(tiles.astype(jnp.float32), axis=0)


def from_everyone(shard):
    copies = jnp.broadcast_to(shard, (lax.axis_size("tp"), *shard.shape))
    return lax.all_to_all(copies, "tp", split_axis=0, concat_axis=0, tiled=True)


def attention_kernel(heads, head_dim, rows, offsets, queries, *refs):
    blocks, out = refs[:-1], refs[-1]
    width = heads * head_dim
    own_docs = blocks[0][rows : rows + 1, :rows].astype(jnp.float32)
    q_docs = jnp.broadcast_to(own_docs, (rows, rows)).T
    q_docs = jnp.concatenate([q_docs, q_docs], axis=1)
    r = lax.broadcasted_iota(jnp.int32, (rows, 2 * rows), 0)
    c = lax.broadcasted_iota(jnp.int32, (rows, 2 * rows), 1)
    causal = c - rows < r
    j = lax.broadcasted_iota(jnp.int32, (2 * rows, 2 * rows), 0)
    s = lax.broadcasted_iota(jnp.int32, (2 * rows, 2 * rows), 1)
    later = (j > s).astype(jnp.float32).astype(jnp.bfloat16)
    totals = [jnp.zeros((rows, head_dim), jnp.float32) for _ in range(heads)]
    carried = [jnp.zeros((rows, 1), jnp.float32) for _ in range(heads)]
    scale = head_dim ** (-0.5)
    for pair in range(len(blocks) // 2):
        near, far = blocks[2 * pair], blocks[2 * pair + 1]
        k_docs = jnp.concatenate([far[rows : rows + 1, :rows], near[rows : rows + 1, :rows]], axis=1)
        live = k_docs.astype(jnp.float32) == q_docs
        if pair == 0:
            live = live & causal
        for h in range(heads):
            cols = slice(h * head_dim, (h + 1) * head_dim)
            v_cols = slice(width + h * head_dim, width + (h + 1) * head_dim)
            k = jnp.concatenate([far[:rows, cols], near[:rows, cols]], axis=0)
            v = jnp.concatenate([far[:rows, v_cols], near[:rows, v_cols]], axis=0)
            z = lax.dot_general(
                queries[:, cols], k, (((1,), (1,)), ((), ())), preferred_element_type=jnp.float32
            ) * scale + offsets[h]
            soft = jnp.log(1.0 + jnp.exp(-jnp.abs(z)))
            keep = jnp.where(live, jnp.minimum(-z, 0.0) - soft, 0.0)
            high = keep.astype(jnp.bfloat16)
            low = (keep - high.astype(jnp.float32)).astype(jnp.bfloat16)
            tail = jnp.dot(high, later, preferred_element_type=jnp.float32) + jnp.dot(
                low, later, preferred_element_type=jnp.float32
            )
            weight = jnp.where(live, jnp.exp(jnp.minimum(z, 0.0) - soft + tail + carried[h]), 0.0)
            totals[h] += jnp.dot(weight.astype(jnp.bfloat16), v, preferred_element_type=jnp.float32)
            carried[h] += tail[:, :1] + keep[:, :1]
    out[...] = jnp.concatenate(totals, axis=1).astype(jnp.bfloat16)


def attention(queries, blocks, offsets):
    rows, width = queries.shape
    heads = offsets.shape[0]
    vmem = pl.BlockSpec(memory_space=pltpu.VMEM)

    def body(*refs):
        attention_kernel(heads, width // heads, rows, *refs)

    return pl.pallas_call(
        body,
        out_shape=jax.ShapeDtypeStruct((rows, width), jnp.bfloat16),
        in_specs=[pl.BlockSpec(memory_space=pltpu.SMEM)] + [vmem] * (1 + len(blocks)),
        out_specs=vmem,
        name="attention",
    )(offsets, queries, *blocks)


def ffn_kernel(parts, place, x, gate_up, *refs):
    downs, out = refs[:parts], refs[parts]
    gu, dn, gu_sems, dn_sems = refs[parts + 1 :]
    units = gu.shape[1] // 2
    step = gu.shape[0] // parts
    wide = dn.shape[1]
    gu_copies = [
        pltpu.make_async_copy(gate_up.at[pl.ds(i * step, step)], gu.at[pl.ds(i * step, step)], gu_sems.at[i])
        for i in range(parts)
    ]
    dn_copies = [pltpu.make_async_copy(downs[i], dn.at[i], dn_sems.at[i]) for i in range(parts)]
    for copy in gu_copies + dn_copies:
        copy.start()
    acc = None
    for i in range(parts):
        gu_copies[i].wait()
        term = jnp.dot(
            x[:, i * step : (i + 1) * step],
            gu[i * step : (i + 1) * step, :],
            preferred_element_type=jnp.float32,
        )
        acc = term if acc is None else acc + term
    gate, upper = acc[:, :units], acc[:, units:]
    hidden = (gate / (1.0 + jnp.exp(-gate)) * upper).astype(jnp.bfloat16)
    for i in range(parts):
        dn_copies[i].wait()
        term = lax.dot_general(
            hidden, dn[i], (((1,), (1,)), ((), ())), preferred_element_type=jnp.float32
        )
        at = pl.multiple_of(place[i] * wide, wide)
        out[:, pl.ds(at, wide)] = term.astype(jnp.bfloat16)


def ffn(x, gate_up, downs, place):
    parts = len(downs)
    wide, units = downs[0].shape
    vmem = pl.BlockSpec(memory_space=pltpu.VMEM)
    hbm = pl.BlockSpec(memory_space=pl.ANY)

    def body(*refs):
        ffn_kernel(parts, *refs)

    return pl.pallas_call(
        body,
        out_shape=jax.ShapeDtypeStruct((x.shape[0], parts * wide), jnp.bfloat16),
        in_specs=[pl.BlockSpec(memory_space=pltpu.SMEM), vmem] + [hbm] * (1 + parts),
        out_specs=vmem,
        scratch_shapes=[
            pltpu.VMEM(gate_up.shape, jnp.bfloat16),
            pltpu.VMEM((parts, wide, units), jnp.bfloat16),
            pltpu.SemaphoreType.DMA((parts,)),
            pltpu.SemaphoreType.DMA((parts,)),
        ],
        name="ffn",
    )(place, x, gate_up, *downs)


def on_device(
    ring,
    resid,
    queries,
    keys,
    values,
    doc_ids,
    score_offset,
    out_weight,
    norm_gain,
    gate_weight,
    up_weight,
    down_weight,
):
    rows = queries.shape[0]
    gate_up = lax.all_gather(
        jnp.concatenate([gate_weight, up_weight], axis=1), "sp", axis=0, tiled=True
    )

    spans = lax.axis_size("sp")
    rings = spans // ring
    groups = [list(range(i * ring, (i + 1) * ring)) for i in range(rings)]
    down = lax.all_gather(down_weight.T, "sp", axis=0, tiled=True, axis_index_groups=groups)
    downs = {0: down}
    for back in range(1, rings // 2 + 1):
        downs[back] = shifted(downs[back - 1], ring)
        if rings - back > rings // 2:
            downs[rings - back] = shifted(downs[(rings - back + 1) % rings], -ring)
    place = (lax.axis_index("sp") // ring - jnp.arange(rings, dtype=jnp.int32)) % rings

    docs = jnp.pad(doc_ids.astype(jnp.bfloat16)[None], ((0, 15), (0, 2 * keys.shape[1] - rows)))
    own = jnp.concatenate([jnp.concatenate([keys, values], axis=1), docs], axis=0)
    blocks = [own] + [shifted(own, back) for back in range(1, 8)]
    attended = attention(queries, blocks, score_offset)

    mixed_attn = summed_for_owner(
        jnp.dot(attended, out_weight, preferred_element_type=jnp.float32).astype(jnp.bfloat16)
    )
    stream = resid.astype(jnp.float32) + mixed_attn
    normed = (
        stream * lax.rsqrt(jnp.mean(stream * stream, axis=1, keepdims=True) + 1e-06) * norm_gain
    ).astype(jnp.bfloat16)
    span_rows = from_everyone(normed).reshape(rows, -1)
    feed = summed_for_owner(ffn(span_rows, gate_up, [downs[i] for i in range(rings)], place))
    return (stream + feed).astype(jnp.bfloat16)


def solution(mesh):
    in_specs = (
        P(("sp", "tp"), None),
        P("sp", "tp"),
        P("sp", "tp"),
        P("sp", "tp"),
        P("sp"),
        P("tp"),
        P("tp", None),
        P(),
        P("sp", "tp"),
        P("sp", "tp"),
        P("tp", "sp"),
    )
    out_specs = P(("sp", "tp"), None)
    return jax.shard_map(
        partial(on_device, 8), mesh=mesh, in_specs=in_specs, out_specs=out_specs, check_vma=False
    )
```

```python
from functools import partial

import jax
import jax.numpy as jnp
from jax import lax
from jax.experimental import pallas as pl
from jax.experimental.pallas import tpu as pltpu
from jax.sharding import PartitionSpec as P


def shifted(block, by):
    spans = lax.axis_size("sp")
    return lax.ppermute(block, "sp", [(i, (i + by) % spans) for i in range(spans)])


def summed_for_owner(terms):
    peers = lax.axis_size("tp")
    tiles = terms.reshape(peers, terms.shape[0] // peers, terms.shape[1])
    tiles = lax.all_to_all(tiles, "tp", 0, 0, tiled=True)
    return jnp.sum(tiles.astype(jnp.float32), axis=0)


def from_everyone(shard):
    copies = jnp.broadcast_to(shard, (lax.axis_size("tp"), *shard.shape))
    return lax.all_to_all(copies, "tp", split_axis=0, concat_axis=0, tiled=True)


def attention_kernel(heads, head_dim, rows, offsets, queries, *refs):
    blocks, out = refs[:-1], refs[-1]
    width = heads * head_dim
    own_docs = blocks[0][rows : rows + 1, :rows].astype(jnp.float32)
    q_docs = jnp.broadcast_to(own_docs, (rows, rows)).T
    q_docs = jnp.concatenate([q_docs, q_docs], axis=1)
    r = lax.broadcasted_iota(jnp.int32, (rows, 2 * rows), 0)
    c = lax.broadcasted_iota(jnp.int32, (rows, 2 * rows), 1)
    causal = c - rows < r
    j = lax.broadcasted_iota(jnp.int32, (2 * rows, 2 * rows), 0)
    s = lax.broadcasted_iota(jnp.int32, (2 * rows, 2 * rows), 1)
    later = (j > s).astype(jnp.float32).astype(jnp.bfloat16)
    totals = [jnp.zeros((rows, head_dim), jnp.float32) for _ in range(heads)]
    carried = [jnp.zeros((rows, 1), jnp.float32) for _ in range(heads)]
    scale = head_dim ** (-0.5)
    for pair in range(len(blocks) // 2):
        near, far = blocks[2 * pair], blocks[2 * pair + 1]
        k_docs = jnp.concatenate([far[rows : rows + 1, :rows], near[rows : rows + 1, :rows]], axis=1)
        live = k_docs.astype(jnp.float32) == q_docs
        if pair == 0:
            live = live & causal
        for h in range(heads):
            cols = slice(h * head_dim, (h + 1) * head_dim)
            v_cols = slice(width + h * head_dim, width + (h + 1) * head_dim)
            k = jnp.concatenate([far[:rows, cols], near[:rows, cols]], axis=0)
            v = jnp.concatenate([far[:rows, v_cols], near[:rows, v_cols]], axis=0)
            z = lax.dot_general(
                queries[:, cols], k, (((1,), (1,)), ((), ())), preferred_element_type=jnp.float32
            ) * scale + offsets[h]
            soft = jnp.log(1.0 + jnp.exp(-jnp.abs(z)))
            keep = jnp.where(live, jnp.minimum(-z, 0.0) - soft, 0.0)
            high = keep.astype(jnp.bfloat16)
            low = (keep - high.astype(jnp.float32)).astype(jnp.bfloat16)
            tail = jnp.dot(high, later, preferred_element_type=jnp.float32) + jnp.dot(
                low, later, preferred_element_type=jnp.float32
            )
            weight = jnp.where(live, jnp.exp(jnp.minimum(z, 0.0) - soft + tail + carried[h]), 0.0)
            totals[h] += jnp.dot(weight.astype(jnp.bfloat16), v, preferred_element_type=jnp.float32)
            carried[h] += tail[:, :1] + keep[:, :1]
    out[...] = jnp.concatenate(totals, axis=1).astype(jnp.bfloat16)


def attention(queries, blocks, offsets):
    rows, width = queries.shape
    heads = offsets.shape[0]
    vmem = pl.BlockSpec(memory_space=pltpu.VMEM)

    def body(*refs):
        attention_kernel(heads, width // heads, rows, *refs)

    return pl.pallas_call(
        body,
        out_shape=jax.ShapeDtypeStruct((rows, width), jnp.bfloat16),
        in_specs=[pl.BlockSpec(memory_space=pltpu.SMEM)] + [vmem] * (1 + len(blocks)),
        out_specs=vmem,
        compiler_params=pltpu.CompilerParams(vmem_limit_bytes=12 << 20),
        name="attention",
    )(offsets, queries, *blocks)


def around(block, pairs, steps):
    got = {0: block}
    for back in range(1, steps // 2 + 1):
        got[back] = lax.ppermute(got[back - 1], "sp", pairs)
        if steps - back > steps // 2:
            got[steps - back] = lax.ppermute(
                got[(steps - back + 1) % steps], "sp", [(j, i) for i, j in pairs]
            )
    return [got[k] for k in range(steps)]


def spread(copies, groups):
    tiles = lax.all_to_all(copies, "sp", 0, 0, tiled=True, axis_index_groups=groups)
    return tiles.reshape(copies.shape[0] * copies.shape[1], copies.shape[2])


def ffn_kernel(ring, low, places, x, *refs):
    first, second, (out, x_turned) = refs[:ring], refs[ring : 2 * ring], refs[2 * ring :]
    step = first[0].shape[0]
    high = first[0].shape[1] - (second[0].shape[1] - low)

    def part(rows, i):
        return rows[:, pl.ds(pl.multiple_of(places[i] * step, step), step)]

    wide = step // ring
    for y in range(ring):
        x_turned[:, y * step : (y + 1) * step] = jnp.concatenate(
            [x[:, z * step + y * wide : z * step + (y + 1) * wide] for z in range(ring)], axis=1
        )
    gate_high = low_up = None
    for k in range(ring):
        one = jnp.dot(part(x, k), first[k][:, :high], preferred_element_type=jnp.float32)
        two = jnp.dot(part(x_turned, ring + k), second[k][...], preferred_element_type=jnp.float32)
        gate_high = one if k == 0 else gate_high + one
        low_up = two if k == 0 else low_up + two
    gate = jnp.concatenate([low_up[:, :low], gate_high], axis=1)
    hidden = (gate / (1.0 + jnp.exp(-gate)) * low_up[:, low:]).astype(jnp.bfloat16)
    for k in range(ring):
        term = lax.dot_general(
            hidden, first[k][:, high:], (((1,), (1,)), ((), ())), preferred_element_type=jnp.float32
        )
        out[:, pl.ds(pl.multiple_of(places[k] * step, step), step)] = term.astype(jnp.bfloat16)


def ffn(x, first, second, places, low):
    ring = len(first)
    vmem = pl.BlockSpec(memory_space=pltpu.VMEM)

    def body(*refs):
        ffn_kernel(ring, low, *refs)

    return pl.pallas_call(
        body,
        out_shape=jax.ShapeDtypeStruct(x.shape, jnp.bfloat16),
        in_specs=[pl.BlockSpec(memory_space=pltpu.SMEM)] + [vmem] * (1 + 2 * ring),
        out_specs=vmem,
        scratch_shapes=[pltpu.VMEM(x.shape, jnp.bfloat16)],
        compiler_params=pltpu.CompilerParams(vmem_limit_bytes=24 << 20),
        name="ffn",
    )(places, x, *first, *second)


def on_device(
    ring,
    resid,
    queries,
    keys,
    values,
    doc_ids,
    score_offset,
    out_weight,
    norm_gain,
    gate_weight,
    up_weight,
    down_weight,
):
    rows = queries.shape[0]
    units = gate_weight.shape[1]
    low = units // 2
    spans = lax.axis_size("sp")
    rings = spans // ring
    along_y = [[z * ring + y for y in range(ring)] for z in range(rings)]
    along_z = [[z * ring + y for z in range(rings)] for y in range(ring)]
    next_y = [(g[i], g[(i + 1) % ring]) for g in along_y for i in range(ring)]
    next_z = [(g[i], g[(i + 1) % rings]) for g in along_z for i in range(rings)]
    first = jnp.concatenate([gate_weight[:, low:], down_weight.T], axis=1)
    second = jnp.concatenate([gate_weight[:, :low], up_weight], axis=1)
    first = jnp.broadcast_to(first, (ring, *first.shape))
    second = jnp.broadcast_to(second, (rings, *second.shape))
    first, second = lax.optimization_barrier((first, second))
    with jax.named_scope("spread_first"):
        first = spread(first, along_y)
    with jax.named_scope("spread_second"):
        second = spread(second, along_z)
    with jax.named_scope("ring_first"):
        first = around(first, next_z, rings)
    with jax.named_scope("ring_second"):
        second = around(second, next_y, ring)
    at = lax.axis_index("sp")
    back = jnp.arange(ring, dtype=jnp.int32)
    places = jnp.concatenate(
        [(at // ring + rings - back) & (rings - 1), ((at & (ring - 1)) + ring - back) & (ring - 1)]
    )

    docs = jnp.pad(doc_ids.astype(jnp.bfloat16)[None], ((0, 15), (0, 2 * keys.shape[1] - rows)))
    own = jnp.concatenate([jnp.concatenate([keys, values], axis=1), docs], axis=0)
    with jax.named_scope("kv_near"):
        near = {k: shifted(own, k) for k in (2, 6, 1, 7)}
    with jax.named_scope("kv_far"):
        far = {4: shifted(near[2], 2), 3: shifted(near[2], 1), 5: shifted(near[6], -1)}
    blocks = {0: own, **near, **far}
    attended = attention(queries, [blocks[b] for b in range(8)], score_offset)

    mixed_attn = summed_for_owner(
        jnp.dot(attended, out_weight, preferred_element_type=jnp.float32).astype(jnp.bfloat16)
    )
    stream = resid.astype(jnp.float32) + mixed_attn
    normed = (
        stream * lax.rsqrt(jnp.mean(stream * stream, axis=1, keepdims=True) + 1e-06) * norm_gain
    ).astype(jnp.bfloat16)
    x = from_everyone(normed).reshape(rows, -1)
    feed = summed_for_owner(ffn(x, first, second, places, low))
    return (stream + feed).astype(jnp.bfloat16)


def solution(mesh):
    in_specs = (
        P(("sp", "tp"), None),
        P("sp", "tp"),
        P("sp", "tp"),
        P("sp", "tp"),
        P("sp"),
        P("tp"),
        P("tp", None),
        P(),
        P("sp", "tp"),
        P("sp", "tp"),
        P("tp", "sp"),
    )
    out_specs = P(("sp", "tp"), None)
    return jax.shard_map(
        partial(on_device, 8), mesh=mesh, in_specs=in_specs, out_specs=out_specs, check_vma=False
    )
```

```python
from functools import partial

import jax
import jax.numpy as jnp
from jax import lax
from jax.experimental import pallas as pl
from jax.experimental.pallas import tpu as pltpu
from jax.sharding import PartitionSpec as P


def shifted(block, by):
    spans = lax.axis_size("sp")
    return lax.ppermute(block, "sp", [(i, (i + by) % spans) for i in range(spans)])


def summed_for_owner(terms):
    peers = lax.axis_size("tp")
    tiles = terms.reshape(peers, terms.shape[0] // peers, terms.shape[1])
    tiles = lax.all_to_all(tiles, "tp", 0, 0, tiled=True)
    return jnp.sum(tiles.astype(jnp.float32), axis=0)


def from_everyone(shard):
    copies = jnp.broadcast_to(shard, (lax.axis_size("tp"), *shard.shape))
    return lax.all_to_all(copies, "tp", split_axis=0, concat_axis=0, tiled=True)


def attention_kernel(heads, head_dim, rows, offsets, queries, *refs):
    blocks, out = refs[:-1], refs[-1]
    width = heads * head_dim
    own_docs = blocks[0][rows : rows + 1, :rows].astype(jnp.float32)
    q_docs = jnp.broadcast_to(own_docs, (rows, rows)).T
    q_docs = jnp.concatenate([q_docs, q_docs], axis=1)
    r = lax.broadcasted_iota(jnp.int32, (rows, 2 * rows), 0)
    c = lax.broadcasted_iota(jnp.int32, (rows, 2 * rows), 1)
    causal = c - rows < r
    j = lax.broadcasted_iota(jnp.int32, (2 * rows, 2 * rows), 0)
    s = lax.broadcasted_iota(jnp.int32, (2 * rows, 2 * rows), 1)
    later = (j > s).astype(jnp.float32).astype(jnp.bfloat16)
    totals = [jnp.zeros((rows, head_dim), jnp.float32) for _ in range(heads)]
    carried = [jnp.zeros((rows, 1), jnp.float32) for _ in range(heads)]
    scale = head_dim ** (-0.5)
    for pair in range(len(blocks) // 2):
        near, far = blocks[2 * pair], blocks[2 * pair + 1]
        k_docs = jnp.concatenate([far[rows : rows + 1, :rows], near[rows : rows + 1, :rows]], axis=1)
        live = k_docs.astype(jnp.float32) == q_docs
        if pair == 0:
            live = live & causal
        for h in range(heads):
            cols = slice(h * head_dim, (h + 1) * head_dim)
            v_cols = slice(width + h * head_dim, width + (h + 1) * head_dim)
            k = jnp.concatenate([far[:rows, cols], near[:rows, cols]], axis=0)
            v = jnp.concatenate([far[:rows, v_cols], near[:rows, v_cols]], axis=0)
            z = lax.dot_general(
                queries[:, cols], k, (((1,), (1,)), ((), ())), preferred_element_type=jnp.float32
            ) * scale + offsets[h]
            soft = jnp.log(1.0 + jnp.exp(-jnp.abs(z)))
            keep = jnp.where(live, jnp.minimum(-z, 0.0) - soft, 0.0)
            high = keep.astype(jnp.bfloat16)
            low = (keep - high.astype(jnp.float32)).astype(jnp.bfloat16)
            tail = jnp.dot(high, later, preferred_element_type=jnp.float32) + jnp.dot(
                low, later, preferred_element_type=jnp.float32
            )
            weight = jnp.where(live, jnp.exp(jnp.minimum(z, 0.0) - soft + tail + carried[h]), 0.0)
            totals[h] += jnp.dot(weight.astype(jnp.bfloat16), v, preferred_element_type=jnp.float32)
            carried[h] += tail[:, :1] + keep[:, :1]
    out[...] = jnp.concatenate(totals, axis=1).astype(jnp.bfloat16)


def attention(queries, blocks, offsets):
    rows, width = queries.shape
    heads = offsets.shape[0]
    vmem = pl.BlockSpec(memory_space=pltpu.VMEM)

    def body(*refs):
        attention_kernel(heads, width // heads, rows, *refs)

    return pl.pallas_call(
        body,
        out_shape=jax.ShapeDtypeStruct((rows, width), jnp.bfloat16),
        in_specs=[pl.BlockSpec(memory_space=pltpu.SMEM)] + [vmem] * (1 + len(blocks)),
        out_specs=vmem,
        compiler_params=pltpu.CompilerParams(vmem_limit_bytes=12 << 20),
        name="attention",
    )(offsets, queries, *blocks)


def turned(groups, by):
    return [(g[i], g[(i + by) % len(g)]) for g in groups for i in range(len(g))]


def neighbours(shard, groups):
    after = lax.ppermute(shard, "sp", turned(groups, -1))
    before = lax.ppermute(shard, "sp", turned(groups, 1))
    middle = lax.ppermute(jnp.concatenate([before, shard, after]), "sp", turned(groups, -3))
    late = lax.ppermute(jnp.concatenate([shard, after]), "sp", turned(groups, 3))
    return jnp.concatenate([shard, after, middle, late, before])


def around(block, groups):
    up, down = turned(groups, 1), turned(groups, -1)
    half = block.shape[0] // 2
    got = {0: block, 8: block}
    for k in range(1, 4):
        got[k] = lax.ppermute(got[k - 1], "sp", up)
        got[8 - k] = lax.ppermute(got[9 - k], "sp", down)
    far = (lax.ppermute(got[3][:half], "sp", up), lax.ppermute(got[5][half:], "sp", down))
    return [got[0], got[1], got[2], got[3], *far, got[5], got[6], got[7]]


def ffn_kernel(ring, low, places, x, *refs):
    first, second = refs[: ring + 1], refs[ring + 1 : 2 * ring + 2]
    out, x_first, x_second = refs[2 * ring + 2 :]
    step = first[0].shape[0]
    half = step // 2
    wide = step // ring
    high = first[0].shape[1] - (second[0].shape[1] - low)
    z, y = places[0], places[ring]
    for i in range(ring):
        cols = slice(i * step, (i + 1) * step)
        own = x[:, cols].astype(jnp.float32)
        x_first[:, cols] = pltpu.roll(own, (step - y * wide) & (step - 1), 1).astype(jnp.bfloat16)
        across = jnp.concatenate(
            [x[:, k * step + i * wide : k * step + (i + 1) * wide] for k in range(ring)], axis=1
        ).astype(jnp.float32)
        x_second[:, cols] = pltpu.roll(across, (step - z * wide) & (step - 1), 1).astype(jnp.bfloat16)

    def pieces(blocks):
        far = ring // 2
        for k in range(ring):
            if k == far:
                yield k, 0, blocks[far]
                yield k, half, blocks[far + 1]
            else:
                yield k, 0, blocks[k if k < far else k + 1]

    def part(rows, i, offset, count):
        return rows[:, pl.ds(pl.multiple_of(places[i] * step + offset, half), count)]

    gate_high = low_up = None
    for k, offset, block in pieces(first):
        rows = part(x_first, k, offset, block.shape[0])
        one = jnp.dot(rows, block[:, :high], preferred_element_type=jnp.float32)
        gate_high = one if gate_high is None else gate_high + one
    for k, offset, block in pieces(second):
        rows = part(x_second, ring + k, offset, block.shape[0])
        two = jnp.dot(rows, block[...], preferred_element_type=jnp.float32)
        low_up = two if low_up is None else low_up + two
    gate = jnp.concatenate([low_up[:, :low], gate_high], axis=1)
    hidden = (gate / (1.0 + jnp.exp(-gate)) * low_up[:, low:]).astype(jnp.bfloat16)
    terms = {}
    for k, offset, block in pieces(first):
        term = lax.dot_general(
            hidden, block[:, high:], (((1,), (1,)), ((), ())), preferred_element_type=jnp.float32
        )
        terms[k] = term if offset == 0 else jnp.concatenate([terms[k], term], axis=1)
    for k in range(ring):
        straight = pltpu.roll(terms[k], y * wide, 1)
        out[:, pl.ds(pl.multiple_of(places[k] * step, step), step)] = straight.astype(jnp.bfloat16)


def ffn(x, first, second, places, ring, low):
    vmem = pl.BlockSpec(memory_space=pltpu.VMEM)

    def body(*refs):
        ffn_kernel(ring, low, *refs)

    return pl.pallas_call(
        body,
        out_shape=jax.ShapeDtypeStruct(x.shape, jnp.bfloat16),
        in_specs=[pl.BlockSpec(memory_space=pltpu.SMEM)] + [vmem] * (3 + 2 * ring),
        out_specs=vmem,
        scratch_shapes=[pltpu.VMEM(x.shape, jnp.bfloat16)] * 2,
        compiler_params=pltpu.CompilerParams(vmem_limit_bytes=24 << 20),
        name="ffn",
    )(places, x, *first, *second)


def on_device(
    ring,
    resid,
    queries,
    keys,
    values,
    doc_ids,
    score_offset,
    out_weight,
    norm_gain,
    gate_weight,
    up_weight,
    down_weight,
):
    rows = queries.shape[0]
    units = gate_weight.shape[1]
    low = units // 2
    spans = lax.axis_size("sp")
    rings = spans // ring
    along_y = [[z * ring + y for y in range(ring)] for z in range(rings)]
    along_z = [[z * ring + y for z in range(rings)] for y in range(ring)]
    first = jnp.concatenate([gate_weight[:, low:], down_weight.T], axis=1)
    second = jnp.concatenate([gate_weight[:, :low], up_weight], axis=1)
    with jax.named_scope("spread_first"):
        first = neighbours(first, along_y)
    with jax.named_scope("spread_second"):
        second = neighbours(second, along_z)
    with jax.named_scope("ring_first"):
        first = around(first, along_z)
    with jax.named_scope("ring_second"):
        second = around(second, along_y)
    at = lax.axis_index("sp")
    back = jnp.arange(ring, dtype=jnp.int32)
    places = jnp.concatenate(
        [(at // ring + rings - back) & (rings - 1), ((at & (ring - 1)) + ring - back) & (ring - 1)]
    )

    docs = jnp.pad(doc_ids.astype(jnp.bfloat16)[None], ((0, 15), (0, 2 * keys.shape[1] - rows)))
    own = jnp.concatenate([jnp.concatenate([keys, values], axis=1), docs], axis=0)
    with jax.named_scope("kv_near"):
        near = {k: shifted(own, k) for k in (2, 6, 1, 7)}
    with jax.named_scope("kv_far"):
        far = {4: shifted(near[2], 2), 3: shifted(near[2], 1), 5: shifted(near[6], -1)}
    blocks = {0: own, **near, **far}
    attended = attention(queries, [blocks[b] for b in range(8)], score_offset)

    mixed_attn = summed_for_owner(
        jnp.dot(attended, out_weight, preferred_element_type=jnp.float32).astype(jnp.bfloat16)
    )
    stream = resid.astype(jnp.float32) + mixed_attn
    normed = (
        stream * lax.rsqrt(jnp.mean(stream * stream, axis=1, keepdims=True) + 1e-06) * norm_gain
    ).astype(jnp.bfloat16)
    x = from_everyone(normed).reshape(rows, -1)
    feed = summed_for_owner(ffn(x, first, second, places, ring, low))
    return (stream + feed).astype(jnp.bfloat16)


def solution(mesh):
    in_specs = (
        P(("sp", "tp"), None),
        P("sp", "tp"),
        P("sp", "tp"),
        P("sp", "tp"),
        P("sp"),
        P("tp"),
        P("tp", None),
        P(),
        P("sp", "tp"),
        P("sp", "tp"),
        P("tp", "sp"),
    )
    out_specs = P(("sp", "tp"), None)
    return jax.shard_map(
        partial(on_device, 8), mesh=mesh, in_specs=in_specs, out_specs=out_specs, check_vma=False
    )
```

```python
import jax
import jax.numpy as jnp
from jax import lax
from jax.experimental import pallas as pl
from jax.experimental.pallas import tpu as pltpu
from jax.sharding import PartitionSpec as P


def shifted(block, by):
    spans = lax.axis_size("sp")
    return lax.ppermute(block, "sp", [(i, (i + by) % spans) for i in range(spans)])


def summed_for_owner(partial):
    peers = lax.axis_size("tp")
    tiles = partial.reshape(peers, partial.shape[0] // peers, partial.shape[1])
    tiles = lax.all_to_all(tiles, "tp", 0, 0, tiled=True)
    return jnp.sum(tiles.astype(jnp.float32), axis=0)


def from_everyone(shard):
    copies = jnp.broadcast_to(shard, (lax.axis_size("tp"), *shard.shape))
    return lax.all_to_all(copies, "tp", split_axis=0, concat_axis=0, tiled=True)


def attention_kernel(heads, head_dim, rows, offsets, queries, *refs):
    blocks, out = refs[:-1], refs[-1]
    width = heads * head_dim
    own_docs = blocks[0][rows : rows + 1, :rows].astype(jnp.float32)
    q_docs = jnp.broadcast_to(own_docs, (rows, rows)).T
    q_docs = jnp.concatenate([q_docs, q_docs], axis=1)
    r = lax.broadcasted_iota(jnp.int32, (rows, 2 * rows), 0)
    c = lax.broadcasted_iota(jnp.int32, (rows, 2 * rows), 1)
    causal = c - rows < r
    j = lax.broadcasted_iota(jnp.int32, (2 * rows, 2 * rows), 0)
    s = lax.broadcasted_iota(jnp.int32, (2 * rows, 2 * rows), 1)
    later = (j > s).astype(jnp.float32).astype(jnp.bfloat16)
    totals = [jnp.zeros((rows, head_dim), jnp.float32) for _ in range(heads)]
    carried = [jnp.zeros((rows, 1), jnp.float32) for _ in range(heads)]
    scale = head_dim ** (-0.5)
    for pair in range(len(blocks) // 2):
        near, far = blocks[2 * pair], blocks[2 * pair + 1]
        k_docs = jnp.concatenate([far[rows : rows + 1, :rows], near[rows : rows + 1, :rows]], axis=1)
        live = k_docs.astype(jnp.float32) == q_docs
        if pair == 0:
            live = live & causal
        for h in range(heads):
            cols = slice(h * head_dim, (h + 1) * head_dim)
            v_cols = slice(width + h * head_dim, width + (h + 1) * head_dim)
            k = jnp.concatenate([far[:rows, cols], near[:rows, cols]], axis=0)
            v = jnp.concatenate([far[:rows, v_cols], near[:rows, v_cols]], axis=0)
            z = lax.dot_general(
                queries[:, cols], k, (((1,), (1,)), ((), ())), preferred_element_type=jnp.float32
            ) * scale + offsets[h]
            soft = jnp.log(1.0 + jnp.exp(-jnp.abs(z)))
            keep = jnp.where(live, jnp.minimum(-z, 0.0) - soft, 0.0)
            high = keep.astype(jnp.bfloat16)
            low = (keep - high.astype(jnp.float32)).astype(jnp.bfloat16)
            tail = jnp.dot(high, later, preferred_element_type=jnp.float32) + jnp.dot(
                low, later, preferred_element_type=jnp.float32
            )
            weight = jnp.where(live, jnp.exp(jnp.minimum(z, 0.0) - soft + tail + carried[h]), 0.0)
            totals[h] += jnp.dot(weight.astype(jnp.bfloat16), v, preferred_element_type=jnp.float32)
            carried[h] += tail[:, :1] + keep[:, :1]
    out[...] = jnp.concatenate(totals, axis=1).astype(jnp.bfloat16)


def attention(queries, blocks, offsets):
    rows, width = queries.shape
    heads = offsets.shape[0]
    vmem = pl.BlockSpec(memory_space=pltpu.VMEM)

    def body(*refs):
        attention_kernel(heads, width // heads, rows, *refs)

    return pl.pallas_call(
        body,
        out_shape=jax.ShapeDtypeStruct((rows, width), jnp.bfloat16),
        in_specs=[pl.BlockSpec(memory_space=pltpu.SMEM)] + [vmem] * (1 + len(blocks)),
        out_specs=vmem,
        compiler_params=pltpu.CompilerParams(vmem_limit_bytes=12 << 20),
        name="attention",
    )(offsets, queries, *blocks)


def ffn_kernel(cuts, x, weights, out, gate_up, down, sems):
    units = down.shape[1]
    copies = [
        pltpu.make_async_copy(
            weights.at[pl.ds(a, b - a), pl.ds(0, 2 * units)], gate_up.at[pl.ds(a, b - a)], sems.at[i]
        )
        for i, (a, b) in enumerate(cuts)
    ]
    copies.append(
        pltpu.make_async_copy(weights.at[:, pl.ds(2 * units, units)], down, sems.at[len(cuts)])
    )
    copies[0].start()
    acc = None
    for i, (a, b) in enumerate(cuts):
        copies[i].wait()
        copies[i + 1].start()
        term = jnp.dot(x[:, a:b], gate_up[a:b, :], preferred_element_type=jnp.float32)
        acc = term if acc is None else acc + term
    gate, upper = acc[:, :units], acc[:, units:]
    hidden = (gate / (1.0 + jnp.exp(-gate)) * upper).astype(jnp.bfloat16)
    copies[-1].wait()
    out[...] = lax.dot_general(
        hidden, down[...], (((1,), (1,)), ((), ())), preferred_element_type=jnp.float32
    ).astype(jnp.bfloat16)


def ffn(x, weights, units):
    width = weights.shape[0]
    cuts = ((0, 3 * width // 8), (3 * width // 8, width))
    vmem = pl.BlockSpec(memory_space=pltpu.VMEM)

    def body(*refs):
        ffn_kernel(cuts, *refs)

    return pl.pallas_call(
        body,
        out_shape=jax.ShapeDtypeStruct(x.shape, jnp.bfloat16),
        in_specs=[vmem, pl.BlockSpec(memory_space=pltpu.HBM)],
        out_specs=vmem,
        scratch_shapes=[
            pltpu.VMEM((width, 2 * units), jnp.bfloat16),
            pltpu.VMEM((width, units), jnp.bfloat16),
            pltpu.SemaphoreType.DMA((len(cuts) + 1,)),
        ],
        compiler_params=pltpu.CompilerParams(vmem_limit_bytes=48 << 20),
        name="ffn",
    )(x, weights)


def on_device(
    resid,
    queries,
    keys,
    values,
    doc_ids,
    score_offset,
    out_weight,
    norm_gain,
    gate_weight,
    up_weight,
    down_weight,
):
    rows = queries.shape[0]
    units = gate_weight.shape[1]
    packed = jnp.concatenate([gate_weight, up_weight, down_weight.T], axis=1)
    weights = lax.all_gather(packed, "sp", axis=0, tiled=True)

    docs = jnp.pad(doc_ids.astype(jnp.bfloat16)[None], ((0, 15), (0, 2 * keys.shape[1] - rows)))
    own = jnp.concatenate([jnp.concatenate([keys, values], axis=1), docs], axis=0)
    near = {k: shifted(own, k) for k in (2, 6, 1, 7)}
    far = {4: shifted(near[2], 2), 3: shifted(near[2], 1), 5: shifted(near[6], -1)}
    blocks = {0: own, **near, **far}
    attended = attention(queries, [blocks[b] for b in range(8)], score_offset)

    mixed_attn = summed_for_owner(
        jnp.dot(attended, out_weight, preferred_element_type=jnp.float32).astype(jnp.bfloat16)
    )
    stream = resid.astype(jnp.float32) + mixed_attn
    normed = (
        stream * lax.rsqrt(jnp.mean(stream * stream, axis=1, keepdims=True) + 1e-06) * norm_gain
    ).astype(jnp.bfloat16)
    span_rows = from_everyone(normed).reshape(rows, -1)
    feed = summed_for_owner(ffn(span_rows, weights, units))
    return (stream + feed).astype(jnp.bfloat16)


def solution(mesh):
    in_specs = (
        P(("sp", "tp"), None),
        P("sp", "tp"),
        P("sp", "tp"),
        P("sp", "tp"),
        P("sp"),
        P("tp"),
        P("tp", None),
        P(),
        P("sp", "tp"),
        P("sp", "tp"),
        P("tp", "sp"),
    )
    out_specs = P(("sp", "tp"), None)
    return jax.shard_map(
        on_device, mesh=mesh, in_specs=in_specs, out_specs=out_specs, check_vma=False
    )
```

```python
import jax
import jax.numpy as jnp
from jax import lax
from jax.experimental import pallas as pl
from jax.experimental.pallas import tpu as pltpu
from jax.sharding import PartitionSpec as P


def shifted(block, by):
    spans = lax.axis_size("sp")
    return lax.ppermute(block, "sp", [(i, (i + by) % spans) for i in range(spans)])


def summed_for_owner(partial):
    peers = lax.axis_size("tp")
    tiles = partial.reshape(peers, partial.shape[0] // peers, partial.shape[1])
    tiles = lax.all_to_all(tiles, "tp", 0, 0, tiled=True)
    return jnp.sum(tiles.astype(jnp.float32), axis=0)


def from_everyone(shard):
    copies = jnp.broadcast_to(shard, (lax.axis_size("tp"), *shard.shape))
    return lax.all_to_all(copies, "tp", split_axis=0, concat_axis=0, tiled=True)


def attention_kernel(heads, head_dim, rows, offsets, queries, *refs):
    blocks, out = refs[:-1], refs[-1]
    width = heads * head_dim
    own_docs = blocks[0][rows : rows + 1, :rows].astype(jnp.float32)
    q_docs = jnp.broadcast_to(own_docs, (rows, rows)).T
    q_docs = jnp.concatenate([q_docs, q_docs], axis=1)
    r = lax.broadcasted_iota(jnp.int32, (rows, 2 * rows), 0)
    c = lax.broadcasted_iota(jnp.int32, (rows, 2 * rows), 1)
    causal = c - rows < r
    j = lax.broadcasted_iota(jnp.int32, (2 * rows, 2 * rows), 0)
    s = lax.broadcasted_iota(jnp.int32, (2 * rows, 2 * rows), 1)
    later = (j > s).astype(jnp.float32).astype(jnp.bfloat16)
    totals = [jnp.zeros((rows, head_dim), jnp.float32) for _ in range(heads)]
    carried = [jnp.zeros((rows, 1), jnp.float32) for _ in range(heads)]
    scale = head_dim ** (-0.5)
    for pair in range(len(blocks) // 2):
        near, far = blocks[2 * pair], blocks[2 * pair + 1]
        k_docs = jnp.concatenate([far[rows : rows + 1, :rows], near[rows : rows + 1, :rows]], axis=1)
        live = k_docs.astype(jnp.float32) == q_docs
        if pair == 0:
            live = live & causal
        for h in range(heads):
            cols = slice(h * head_dim, (h + 1) * head_dim)
            v_cols = slice(width + h * head_dim, width + (h + 1) * head_dim)
            k = jnp.concatenate([far[:rows, cols], near[:rows, cols]], axis=0)
            v = jnp.concatenate([far[:rows, v_cols], near[:rows, v_cols]], axis=0)
            z = lax.dot_general(
                queries[:, cols], k, (((1,), (1,)), ((), ())), preferred_element_type=jnp.float32
            ) * scale + offsets[h]
            soft = jnp.log(1.0 + jnp.exp(-jnp.abs(z)))
            keep = jnp.where(live, jnp.minimum(-z, 0.0) - soft, 0.0)
            high = keep.astype(jnp.bfloat16)
            low = (keep - high.astype(jnp.float32)).astype(jnp.bfloat16)
            tail = jnp.dot(high, later, preferred_element_type=jnp.float32) + jnp.dot(
                low, later, preferred_element_type=jnp.float32
            )
            weight = jnp.where(live, jnp.exp(jnp.minimum(z, 0.0) - soft + tail + carried[h]), 0.0)
            totals[h] += jnp.dot(weight.astype(jnp.bfloat16), v, preferred_element_type=jnp.float32)
            carried[h] += tail[:, :1] + keep[:, :1]
    out[...] = jnp.concatenate(totals, axis=1).astype(jnp.bfloat16)


def attention(queries, blocks, offsets):
    rows, width = queries.shape
    heads = offsets.shape[0]
    vmem = pl.BlockSpec(memory_space=pltpu.VMEM)

    def body(*refs):
        attention_kernel(heads, width // heads, rows, *refs)

    return pl.pallas_call(
        body,
        out_shape=jax.ShapeDtypeStruct((rows, width), jnp.bfloat16),
        in_specs=[pl.BlockSpec(memory_space=pltpu.SMEM)] + [vmem] * (1 + len(blocks)),
        out_specs=vmem,
        compiler_params=pltpu.CompilerParams(vmem_limit_bytes=12 << 20),
        name="attention",
    )(offsets, queries, *blocks)


def ffn_kernel(cuts, ahead, x, weights, out, gate_up, down, sems):
    units = down.shape[1]
    half = down.shape[0] // 2

    def copy(source, target, sem):
        return pltpu.make_async_copy(source, target, sem)

    stages = []
    for i, (a, b) in enumerate(cuts):
        n = (b - a) // 2
        stages.append(
            [
                copy(
                    weights.at[pl.ds(at, n), pl.ds(0, 2 * units)],
                    gate_up.at[pl.ds(at, n)],
                    sems.at[2 * i + j],
                )
                for j, at in enumerate((a, a + n))
            ]
        )
    for j in range(2):
        rows = pl.ds(j * half, half)
        stages.append(
            [copy(weights.at[rows, pl.ds(2 * units, units)], down.at[rows], sems.at[2 * len(cuts) + j])]
        )

    def start(i):
        for one in stages[i] if i < len(stages) else ():
            one.start()

    def wait(i):
        for one in stages[i]:
            one.wait()
        start(i + ahead)

    for i in range(ahead):
        start(i)
    acc = None
    for i, (a, b) in enumerate(cuts):
        wait(i)
        term = jnp.dot(x[:, a:b], gate_up[a:b, :], preferred_element_type=jnp.float32)
        acc = term if acc is None else acc + term
    gate, upper = acc[:, :units], acc[:, units:]
    hidden = (gate / (1.0 + jnp.exp(-gate)) * upper).astype(jnp.bfloat16)
    for j in range(2):
        wait(len(cuts) + j)
        rows = slice(j * half, (j + 1) * half)
        out[:, rows] = lax.dot_general(
            hidden, down[rows, :], (((1,), (1,)), ((), ())), preferred_element_type=jnp.float32
        ).astype(jnp.bfloat16)


def ffn(x, weights, units):
    width = weights.shape[0]
    marks = (0, 3 * width // 8, 11 * width // 16, width)
    cuts = tuple(zip(marks[:-1], marks[1:]))
    vmem = pl.BlockSpec(memory_space=pltpu.VMEM)

    def body(*refs):
        ffn_kernel(cuts, 3, *refs)

    return pl.pallas_call(
        body,
        out_shape=jax.ShapeDtypeStruct(x.shape, jnp.bfloat16),
        in_specs=[vmem, pl.BlockSpec(memory_space=pltpu.HBM)],
        out_specs=vmem,
        scratch_shapes=[
            pltpu.VMEM((width, 2 * units), jnp.bfloat16),
            pltpu.VMEM((width, units), jnp.bfloat16),
            pltpu.SemaphoreType.DMA((2 * len(cuts) + 2,)),
        ],
        compiler_params=pltpu.CompilerParams(vmem_limit_bytes=48 << 20),
        name="ffn",
    )(x, weights)


def on_device(
    resid,
    queries,
    keys,
    values,
    doc_ids,
    score_offset,
    out_weight,
    norm_gain,
    gate_weight,
    up_weight,
    down_weight,
):
    rows = queries.shape[0]
    units = gate_weight.shape[1]
    packed = jnp.concatenate([gate_weight, up_weight, down_weight.T], axis=1)
    weights = lax.all_gather(packed, "sp", axis=0, tiled=True)

    docs = jnp.pad(doc_ids.astype(jnp.bfloat16)[None], ((0, 15), (0, 2 * keys.shape[1] - rows)))
    own = jnp.concatenate([jnp.concatenate([keys, values], axis=1), docs], axis=0)
    blocks = {0: own}
    blocks[7] = shifted(own, 7)
    for back in range(1, 5):
        blocks[back] = shifted(blocks[back - 1], 1)
        if back < 3:
            blocks[7 - back] = shifted(blocks[8 - back], -1)
    attended = attention(queries, [blocks[b] for b in range(8)], score_offset)

    mixed_attn = summed_for_owner(
        jnp.dot(attended, out_weight, preferred_element_type=jnp.float32).astype(jnp.bfloat16)
    )
    stream = resid.astype(jnp.float32) + mixed_attn
    normed = (
        stream * lax.rsqrt(jnp.mean(stream * stream, axis=1, keepdims=True) + 1e-06) * norm_gain
    ).astype(jnp.bfloat16)
    span_rows = from_everyone(normed).reshape(rows, -1)
    feed = summed_for_owner(ffn(span_rows, weights, units))
    return (stream + feed).astype(jnp.bfloat16)


def solution(mesh):
    in_specs = (
        P(("sp", "tp"), None),
        P("sp", "tp"),
        P("sp", "tp"),
        P("sp", "tp"),
        P("sp"),
        P("tp"),
        P("tp", None),
        P(),
        P("sp", "tp"),
        P("sp", "tp"),
        P("tp", "sp"),
    )
    out_specs = P(("sp", "tp"), None)
    return jax.shard_map(
        on_device, mesh=mesh, in_specs=in_specs, out_specs=out_specs, check_vma=False
    )
```

```python
import jax
import jax.numpy as jnp
from jax import lax
from jax.experimental import pallas as pl
from jax.experimental.pallas import tpu as pltpu
from jax.sharding import PartitionSpec as P


def shifted(block, by):
    spans = lax.axis_size("sp")
    return lax.ppermute(block, "sp", [(i, (i + by) % spans) for i in range(spans)])


def summed_for_owner(partial):
    peers = lax.axis_size("tp")
    tiles = partial.reshape(peers, partial.shape[0] // peers, partial.shape[1])
    tiles = lax.all_to_all(tiles, "tp", 0, 0, tiled=True)
    return jnp.sum(tiles.astype(jnp.float32), axis=0)


def from_everyone(shard):
    copies = jnp.broadcast_to(shard, (lax.axis_size("tp"), *shard.shape))
    return lax.all_to_all(copies, "tp", split_axis=0, concat_axis=0, tiled=True)


def attention_kernel(heads, head_dim, rows, offsets, queries, *refs):
    blocks, out = refs[:-1], refs[-1]
    width = heads * head_dim
    own_docs = blocks[0][rows : rows + 1, :rows].astype(jnp.float32)
    q_docs = jnp.broadcast_to(own_docs, (rows, rows)).T
    q_docs = jnp.concatenate([q_docs, q_docs], axis=1)
    r = lax.broadcasted_iota(jnp.int32, (rows, 2 * rows), 0)
    c = lax.broadcasted_iota(jnp.int32, (rows, 2 * rows), 1)
    causal = c - rows < r
    j = lax.broadcasted_iota(jnp.int32, (2 * rows, 2 * rows), 0)
    s = lax.broadcasted_iota(jnp.int32, (2 * rows, 2 * rows), 1)
    later = (j > s).astype(jnp.float32).astype(jnp.bfloat16)
    totals = [jnp.zeros((rows, head_dim), jnp.float32) for _ in range(heads)]
    carried = [jnp.zeros((rows, 1), jnp.float32) for _ in range(heads)]
    scale = head_dim ** (-0.5)
    for pair in range(len(blocks) // 2):
        near, far = blocks[2 * pair], blocks[2 * pair + 1]
        k_docs = jnp.concatenate([far[rows : rows + 1, :rows], near[rows : rows + 1, :rows]], axis=1)
        live = k_docs.astype(jnp.float32) == q_docs
        if pair == 0:
            live = live & causal
        for h in range(heads):
            cols = slice(h * head_dim, (h + 1) * head_dim)
            v_cols = slice(width + h * head_dim, width + (h + 1) * head_dim)
            k = jnp.concatenate([far[:rows, cols], near[:rows, cols]], axis=0)
            v = jnp.concatenate([far[:rows, v_cols], near[:rows, v_cols]], axis=0)
            z = lax.dot_general(
                queries[:, cols], k, (((1,), (1,)), ((), ())), preferred_element_type=jnp.float32
            ) * scale + offsets[h]
            soft = jnp.log(1.0 + jnp.exp(-jnp.abs(z)))
            keep = jnp.where(live, jnp.minimum(-z, 0.0) - soft, 0.0)
            high = keep.astype(jnp.bfloat16)
            low = (keep - high.astype(jnp.float32)).astype(jnp.bfloat16)
            tail = jnp.dot(high, later, preferred_element_type=jnp.float32) + jnp.dot(
                low, later, preferred_element_type=jnp.float32
            )
            weight = jnp.where(live, jnp.exp(jnp.minimum(z, 0.0) - soft + tail + carried[h]), 0.0)
            totals[h] += jnp.dot(weight.astype(jnp.bfloat16), v, preferred_element_type=jnp.float32)
            carried[h] += tail[:, :1] + keep[:, :1]
    out[...] = jnp.concatenate(totals, axis=1).astype(jnp.bfloat16)


def attention(queries, blocks, offsets):
    rows, width = queries.shape
    heads = offsets.shape[0]
    vmem = pl.BlockSpec(memory_space=pltpu.VMEM)

    def body(*refs):
        attention_kernel(heads, width // heads, rows, *refs)

    return pl.pallas_call(
        body,
        out_shape=jax.ShapeDtypeStruct((rows, width), jnp.bfloat16),
        in_specs=[pl.BlockSpec(memory_space=pltpu.SMEM)] + [vmem] * (1 + len(blocks)),
        out_specs=vmem,
        compiler_params=pltpu.CompilerParams(vmem_limit_bytes=12 << 20),
        name="attention",
    )(offsets, queries, *blocks)


def ffn_kernel(cuts, ahead, x, gate_low, weights, out, gate_up, down, sems):
    units = down.shape[1]
    half = down.shape[0] // 2
    wide = gate_up.shape[1]

    def copy(source, target, sem):
        return pltpu.make_async_copy(source, target, sem)

    stages = []
    for i, (a, b) in enumerate(cuts):
        n = (b - a) // 2
        stages.append(
            [
                copy(
                    weights.at[pl.ds(at, n), pl.ds(0, wide)],
                    gate_up.at[pl.ds(at, n)],
                    sems.at[2 * i + j],
                )
                for j, at in enumerate((a, a + n))
            ]
        )
    for j in range(2):
        rows = pl.ds(j * half, half)
        stages.append(
            [copy(weights.at[rows, pl.ds(wide, units)], down.at[rows], sems.at[2 * len(cuts) + j])]
        )

    def start(i):
        for one in stages[i] if i < len(stages) else ():
            one.start()

    def wait(i):
        for one in stages[i]:
            one.wait()
        start(i + ahead)

    for i in range(ahead):
        start(i)
    acc = None
    for i, (a, b) in enumerate(cuts):
        wait(i)
        term = jnp.dot(x[:, a:b], gate_up[a:b, :], preferred_element_type=jnp.float32)
        acc = term if acc is None else acc + term
    gate = jnp.concatenate([gate_low[...], acc[:, : wide - units]], axis=1)
    upper = acc[:, wide - units :]
    hidden = (gate / (1.0 + jnp.exp(-gate)) * upper).astype(jnp.bfloat16)
    for j in range(2):
        wait(len(cuts) + j)
        rows = slice(j * half, (j + 1) * half)
        out[:, rows] = lax.dot_general(
            hidden, down[rows, :], (((1,), (1,)), ((), ())), preferred_element_type=jnp.float32
        ).astype(jnp.bfloat16)


def ffn(x, gate_low, weights, units):
    width = weights.shape[0]
    wide = weights.shape[1] - units
    marks = (0, 3 * width // 8, 11 * width // 16, width)
    cuts = tuple(zip(marks[:-1], marks[1:]))
    vmem = pl.BlockSpec(memory_space=pltpu.VMEM)

    def body(*refs):
        ffn_kernel(cuts, 3, *refs)

    return pl.pallas_call(
        body,
        out_shape=jax.ShapeDtypeStruct(x.shape, jnp.bfloat16),
        in_specs=[vmem, vmem, pl.BlockSpec(memory_space=pltpu.HBM)],
        out_specs=vmem,
        scratch_shapes=[
            pltpu.VMEM((width, wide), jnp.bfloat16),
            pltpu.VMEM((width, units), jnp.bfloat16),
            pltpu.SemaphoreType.DMA((2 * len(cuts) + 2,)),
        ],
        compiler_params=pltpu.CompilerParams(vmem_limit_bytes=48 << 20),
        name="ffn",
    )(x, gate_low, weights)


def side_kernel(start, x, *refs):
    blocks, out = refs[:-1], refs[-1]
    step = blocks[0].shape[0]
    width = x.shape[1]
    turned = pltpu.roll(x[...].astype(jnp.float32), (width - start[0]) & (width - 1), 1)
    turned = turned.astype(jnp.bfloat16)
    acc = None
    for i in range(len(blocks)):
        term = jnp.dot(
            turned[:, i * step : (i + 1) * step],
            blocks[len(blocks) - 1 - i][...],
            preferred_element_type=jnp.float32,
        )
        acc = term if acc is None else acc + term
    out[...] = acc


def side(x, blocks, start):
    vmem = pl.BlockSpec(memory_space=pltpu.VMEM)
    return pl.pallas_call(
        side_kernel,
        out_shape=jax.ShapeDtypeStruct((x.shape[0], blocks[0].shape[1]), jnp.float32),
        in_specs=[pl.BlockSpec(memory_space=pltpu.SMEM)] + [vmem] * (1 + len(blocks)),
        out_specs=vmem,
        compiler_params=pltpu.CompilerParams(vmem_limit_bytes=12 << 20),
        name="side",
    )(start, x, *blocks)


def on_device(
    resid,
    queries,
    keys,
    values,
    doc_ids,
    score_offset,
    out_weight,
    norm_gain,
    gate_weight,
    up_weight,
    down_weight,
):
    rows = queries.shape[0]
    units = gate_weight.shape[1]
    low = units // 2
    packed = jnp.concatenate([gate_weight[:, low:], up_weight, down_weight.T], axis=1)
    weights = lax.all_gather(packed, "sp", axis=0, tiled=True)

    docs = jnp.pad(doc_ids.astype(jnp.bfloat16)[None], ((0, 15), (0, 2 * keys.shape[1] - rows)))
    shard = jnp.pad(gate_weight[:, :low], ((0, 0), (0, 2 * keys.shape[1] - low)))
    tall = rows + docs.shape[0]
    own = jnp.concatenate([jnp.concatenate([keys, values], axis=1), docs])
    both = jnp.concatenate([own, shard])
    blocks = {0: both}
    blocks[1] = shifted(both, 1)
    blocks[7] = shifted(own, 7)
    after = shifted(shard, -1)
    blocks[2] = shifted(blocks[1], 1)
    blocks[6] = shifted(jnp.concatenate([blocks[7], after]), -1)
    blocks[3] = shifted(blocks[2], 1)
    blocks[5] = shifted(blocks[6], -1)
    blocks[4] = shifted(blocks[3], 1)
    near = [blocks[k][tall:, :low] for k in (4, 3, 2, 1)]
    near += [shard[:, :low], after[:, :low]] + [blocks[k][tall:, :low] for k in (6, 5)]
    ring, rings = len(near), lax.axis_size("sp") // len(near)
    sides = {0: jnp.concatenate(near)}
    for k in range(1, rings // 2 + 1):
        sides[k] = shifted(sides[k - 1], ring)
        if k < rings // 2:
            sides[rings - k] = shifted(sides[(rings - k + 1) % rings], -ring)
    start = ((lax.axis_index("sp") + ring // 2) & (ring * rings - 1)) * near[0].shape[0]
    attended = attention(queries, [blocks[b] for b in range(8)], score_offset)

    mixed_attn = summed_for_owner(
        jnp.dot(attended, out_weight, preferred_element_type=jnp.float32).astype(jnp.bfloat16)
    )
    stream = resid.astype(jnp.float32) + mixed_attn
    normed = (
        stream * lax.rsqrt(jnp.mean(stream * stream, axis=1, keepdims=True) + 1e-06) * norm_gain
    ).astype(jnp.bfloat16)
    span_rows = from_everyone(normed).reshape(rows, -1)
    gate_low = side(span_rows, [sides[k] for k in range(rings)], start[None])
    feed = summed_for_owner(ffn(span_rows, gate_low, weights, units))
    return (stream + feed).astype(jnp.bfloat16)


def solution(mesh):
    in_specs = (
        P(("sp", "tp"), None),
        P("sp", "tp"),
        P("sp", "tp"),
        P("sp", "tp"),
        P("sp"),
        P("tp"),
        P("tp", None),
        P(),
        P("sp", "tp"),
        P("sp", "tp"),
        P("tp", "sp"),
    )
    out_specs = P(("sp", "tp"), None)

    return jax.shard_map(
        on_device, mesh=mesh, in_specs=in_specs, out_specs=out_specs, check_vma=False
    )
```

```python
import jax
import jax.numpy as jnp
from jax import lax
from jax.experimental import pallas as pl
from jax.experimental.pallas import tpu as pltpu
from jax.sharding import PartitionSpec as P


def shifted(block, by):
    spans = lax.axis_size("sp")
    return lax.ppermute(block, "sp", [(i, (i + by) % spans) for i in range(spans)])


def summed_for_owner(partial):
    peers = lax.axis_size("tp")
    tiles = partial.reshape(peers, partial.shape[0] // peers, partial.shape[1])
    tiles = lax.all_to_all(tiles, "tp", 0, 0, tiled=True)
    return jnp.sum(tiles.astype(jnp.float32), axis=0)


def from_everyone(shard):
    copies = jnp.broadcast_to(shard, (lax.axis_size("tp"), *shard.shape))
    return lax.all_to_all(copies, "tp", split_axis=0, concat_axis=0, tiled=True)


def attention_kernel(heads, head_dim, rows, offsets, queries, *refs):
    blocks, out = refs[:-1], refs[-1]
    width = heads * head_dim
    own_docs = blocks[0][rows : rows + 1, :rows].astype(jnp.float32)
    q_docs = jnp.broadcast_to(own_docs, (rows, rows)).T
    q_docs = jnp.concatenate([q_docs, q_docs], axis=1)
    r = lax.broadcasted_iota(jnp.int32, (rows, 2 * rows), 0)
    c = lax.broadcasted_iota(jnp.int32, (rows, 2 * rows), 1)
    causal = c - rows < r
    j = lax.broadcasted_iota(jnp.int32, (2 * rows, 2 * rows), 0)
    s = lax.broadcasted_iota(jnp.int32, (2 * rows, 2 * rows), 1)
    later = (j > s).astype(jnp.float32).astype(jnp.bfloat16)
    totals = [jnp.zeros((rows, head_dim), jnp.float32) for _ in range(heads)]
    carried = [jnp.zeros((rows, 1), jnp.float32) for _ in range(heads)]
    scale = head_dim ** (-0.5)
    for pair in range(len(blocks) // 2):
        near, far = blocks[2 * pair], blocks[2 * pair + 1]
        k_docs = jnp.concatenate([far[rows : rows + 1, :rows], near[rows : rows + 1, :rows]], axis=1)
        live = k_docs.astype(jnp.float32) == q_docs
        if pair == 0:
            live = live & causal
        for h in range(heads):
            cols = slice(h * head_dim, (h + 1) * head_dim)
            v_cols = slice(width + h * head_dim, width + (h + 1) * head_dim)
            k = jnp.concatenate([far[:rows, cols], near[:rows, cols]], axis=0)
            v = jnp.concatenate([far[:rows, v_cols], near[:rows, v_cols]], axis=0)
            z = lax.dot_general(
                queries[:, cols], k, (((1,), (1,)), ((), ())), preferred_element_type=jnp.float32
            ) * scale + offsets[h]
            soft = jnp.log(1.0 + jnp.exp(-jnp.abs(z)))
            keep = jnp.where(live, jnp.minimum(-z, 0.0) - soft, 0.0)
            high = keep.astype(jnp.bfloat16)
            low = (keep - high.astype(jnp.float32)).astype(jnp.bfloat16)
            tail = jnp.dot(high, later, preferred_element_type=jnp.float32) + jnp.dot(
                low, later, preferred_element_type=jnp.float32
            )
            weight = jnp.where(live, jnp.exp(jnp.minimum(z, 0.0) - soft + tail + carried[h]), 0.0)
            totals[h] += jnp.dot(weight.astype(jnp.bfloat16), v, preferred_element_type=jnp.float32)
            carried[h] += tail[:, :1] + keep[:, :1]
    out[...] = jnp.concatenate(totals, axis=1).astype(jnp.bfloat16)


def attention(queries, blocks, offsets):
    rows, width = queries.shape
    heads = offsets.shape[0]
    vmem = pl.BlockSpec(memory_space=pltpu.VMEM)

    def body(*refs):
        attention_kernel(heads, width // heads, rows, *refs)

    return pl.pallas_call(
        body,
        out_shape=jax.ShapeDtypeStruct((rows, width), jnp.bfloat16),
        in_specs=[pl.BlockSpec(memory_space=pltpu.SMEM)] + [vmem] * (1 + len(blocks)),
        out_specs=vmem,
        compiler_params=pltpu.CompilerParams(vmem_limit_bytes=12 << 20),
        name="attention",
    )(offsets, queries, *blocks)


def ffn_kernel(cuts, ahead, x, gate_low, weights, out, gate_up, down, sems):
    units = down.shape[1]
    half = down.shape[0] // 2
    wide = gate_up.shape[1]

    def copy(source, target, sem):
        return pltpu.make_async_copy(source, target, sem)

    stages = []
    for i, (a, b) in enumerate(cuts):
        n = (b - a) // 2
        stages.append(
            [
                copy(
                    weights.at[pl.ds(at, n), pl.ds(0, wide)],
                    gate_up.at[pl.ds(at, n)],
                    sems.at[2 * i + j],
                )
                for j, at in enumerate((a, a + n))
            ]
        )
    for j in range(2):
        rows = pl.ds(j * half, half)
        stages.append(
            [copy(weights.at[rows, pl.ds(wide, units)], down.at[rows], sems.at[2 * len(cuts) + j])]
        )

    def start(i):
        for one in stages[i] if i < len(stages) else ():
            one.start()

    def wait(i):
        for one in stages[i]:
            one.wait()
        start(i + ahead)

    for i in range(ahead):
        start(i)
    acc = None
    for i, (a, b) in enumerate(cuts):
        wait(i)
        term = jnp.dot(x[:, a:b], gate_up[a:b, :], preferred_element_type=jnp.float32)
        acc = term if acc is None else acc + term
    gate = jnp.concatenate([gate_low[...], acc[:, : wide - units]], axis=1)
    upper = acc[:, wide - units :]
    hidden = (gate / (1.0 + jnp.exp(-gate)) * upper).astype(jnp.bfloat16)
    for j in range(2):
        wait(len(cuts) + j)
        rows = slice(j * half, (j + 1) * half)
        out[:, rows] = lax.dot_general(
            hidden, down[rows, :], (((1,), (1,)), ((), ())), preferred_element_type=jnp.float32
        ).astype(jnp.bfloat16)


def ffn(x, gate_low, weights, units):
    width = weights.shape[0]
    wide = weights.shape[1] - units
    marks = (0, 3 * width // 8, 11 * width // 16, width)
    cuts = tuple(zip(marks[:-1], marks[1:]))
    vmem = pl.BlockSpec(memory_space=pltpu.VMEM)

    def body(*refs):
        ffn_kernel(cuts, 3, *refs)

    return pl.pallas_call(
        body,
        out_shape=jax.ShapeDtypeStruct(x.shape, jnp.bfloat16),
        in_specs=[vmem, vmem, pl.BlockSpec(memory_space=pltpu.HBM)],
        out_specs=vmem,
        scratch_shapes=[
            pltpu.VMEM((width, wide), jnp.bfloat16),
            pltpu.VMEM((width, units), jnp.bfloat16),
            pltpu.SemaphoreType.DMA((2 * len(cuts) + 2,)),
        ],
        compiler_params=pltpu.CompilerParams(vmem_limit_bytes=48 << 20),
        name="ffn",
    )(x, gate_low, weights)


def side_kernel(places, x, *refs):
    blocks, out = refs[:-1], refs[-1]
    step = blocks[0].shape[0]
    acc = None
    for k in range(len(blocks)):
        part = x[:, pl.ds(pl.multiple_of(places[k] * step, step), step)]
        term = jnp.dot(part, blocks[k][...], preferred_element_type=jnp.float32)
        acc = term if acc is None else acc + term
    out[...] = acc


def side(x, blocks, places):
    vmem = pl.BlockSpec(memory_space=pltpu.VMEM)
    return pl.pallas_call(
        side_kernel,
        out_shape=jax.ShapeDtypeStruct((x.shape[0], blocks[0].shape[1]), jnp.float32),
        in_specs=[pl.BlockSpec(memory_space=pltpu.SMEM)] + [vmem] * (1 + len(blocks)),
        out_specs=vmem,
        compiler_params=pltpu.CompilerParams(vmem_limit_bytes=12 << 20),
        name="side",
    )(places, x, *blocks)


def on_device(
    resid,
    queries,
    keys,
    values,
    doc_ids,
    score_offset,
    out_weight,
    norm_gain,
    gate_weight,
    up_weight,
    down_weight,
):
    rows = queries.shape[0]
    units = gate_weight.shape[1]
    low = units // 2
    packed = jnp.concatenate([gate_weight[:, low:], up_weight, down_weight.T], axis=1)
    weights = lax.all_gather(packed, "sp", axis=0, tiled=True)

    docs = jnp.pad(doc_ids.astype(jnp.bfloat16)[None], ((0, 15), (0, 2 * keys.shape[1] - rows)))
    own = jnp.concatenate([jnp.concatenate([keys, values], axis=1), docs])
    ring = 8
    rings = lax.axis_size("sp") // ring
    blocks, sides = {0: own}, {}
    blocks[1], blocks[7] = shifted(own, 1), shifted(own, 7)
    shard = gate_weight[:, :low]
    copies = jnp.broadcast_to(shard, (ring, *shard.shape))
    groups = [list(range(i * ring, (i + 1) * ring)) for i in range(rings)]
    tiles = lax.all_to_all(copies, "sp", 0, 0, tiled=True, axis_index_groups=groups)
    sides[0] = tiles.reshape(ring * shard.shape[0], low)
    for k in range(1, rings // 2 + 1):
        sides[k] = shifted(sides[k - 1], ring)
        if k < rings // 2:
            sides[rings - k] = shifted(sides[(rings - k + 1) % rings], -ring)
    for k in range(2, 5):
        blocks[k] = shifted(blocks[k - 1], 1)
        if k < 4:
            blocks[8 - k] = shifted(blocks[9 - k], -1)
    back = jnp.arange(rings, dtype=jnp.int32)
    places = (lax.axis_index("sp") // ring + rings - back) & (rings - 1)
    attended = attention(queries, [blocks[b] for b in range(8)], score_offset)

    mixed_attn = summed_for_owner(
        jnp.dot(attended, out_weight, preferred_element_type=jnp.float32).astype(jnp.bfloat16)
    )
    stream = resid.astype(jnp.float32) + mixed_attn
    normed = (
        stream * lax.rsqrt(jnp.mean(stream * stream, axis=1, keepdims=True) + 1e-06) * norm_gain
    ).astype(jnp.bfloat16)
    span_rows = from_everyone(normed).reshape(rows, -1)
    gate_low = side(span_rows, [sides[k] for k in range(rings)], places)
    feed = summed_for_owner(ffn(span_rows, gate_low, weights, units))
    return (stream + feed).astype(jnp.bfloat16)


def solution(mesh):
    in_specs = (
        P(("sp", "tp"), None),
        P("sp", "tp"),
        P("sp", "tp"),
        P("sp", "tp"),
        P("sp"),
        P("tp"),
        P("tp", None),
        P(),
        P("sp", "tp"),
        P("sp", "tp"),
        P("tp", "sp"),
    )
    out_specs = P(("sp", "tp"), None)

    return jax.shard_map(
        on_device, mesh=mesh, in_specs=in_specs, out_specs=out_specs, check_vma=False
    )
```

```python
import jax
import jax.numpy as jnp
from jax import lax
from jax.experimental import pallas as pl
from jax.experimental.pallas import tpu as pltpu
from jax.sharding import PartitionSpec as P


def shifted(block, by):
    spans = lax.axis_size("sp")
    return lax.ppermute(block, "sp", [(i, (i + by) % spans) for i in range(spans)])


def summed_for_owner(partial):
    peers = lax.axis_size("tp")
    tiles = partial.reshape(peers, partial.shape[0] // peers, partial.shape[1])
    tiles = lax.all_to_all(tiles, "tp", 0, 0, tiled=True)
    return jnp.sum(tiles.astype(jnp.float32), axis=0)


def from_everyone(shard):
    copies = jnp.broadcast_to(shard, (lax.axis_size("tp"), *shard.shape))
    return lax.all_to_all(copies, "tp", split_axis=0, concat_axis=0, tiled=True)


def attention_kernel(heads, head_dim, rows, offsets, queries, *refs):
    blocks, out = refs[:-1], refs[-1]
    width = heads * head_dim
    own_docs = blocks[0][rows : rows + 1, :rows].astype(jnp.float32)
    q_docs = jnp.broadcast_to(own_docs, (rows, rows)).T
    q_docs = jnp.concatenate([q_docs, q_docs], axis=1)
    r = lax.broadcasted_iota(jnp.int32, (rows, 2 * rows), 0)
    c = lax.broadcasted_iota(jnp.int32, (rows, 2 * rows), 1)
    causal = c - rows < r
    j = lax.broadcasted_iota(jnp.int32, (2 * rows, 2 * rows), 0)
    s = lax.broadcasted_iota(jnp.int32, (2 * rows, 2 * rows), 1)
    later = (j > s).astype(jnp.float32).astype(jnp.bfloat16)
    totals = [jnp.zeros((rows, head_dim), jnp.float32) for _ in range(heads)]
    carried = [jnp.zeros((rows, 1), jnp.float32) for _ in range(heads)]
    scale = head_dim ** (-0.5)
    for pair in range(len(blocks) // 2):
        near, far = blocks[2 * pair], blocks[2 * pair + 1]
        k_docs = jnp.concatenate([far[rows : rows + 1, :rows], near[rows : rows + 1, :rows]], axis=1)
        live = k_docs.astype(jnp.float32) == q_docs
        if pair == 0:
            live = live & causal
        for h in range(heads):
            cols = slice(h * head_dim, (h + 1) * head_dim)
            v_cols = slice(width + h * head_dim, width + (h + 1) * head_dim)
            k = jnp.concatenate([far[:rows, cols], near[:rows, cols]], axis=0)
            v = jnp.concatenate([far[:rows, v_cols], near[:rows, v_cols]], axis=0)
            z = lax.dot_general(
                queries[:, cols], k, (((1,), (1,)), ((), ())), preferred_element_type=jnp.float32
            ) * scale + offsets[h]
            soft = jnp.log(1.0 + jnp.exp(-jnp.abs(z)))
            keep = jnp.where(live, jnp.minimum(-z, 0.0) - soft, 0.0)
            high = keep.astype(jnp.bfloat16)
            low = (keep - high.astype(jnp.float32)).astype(jnp.bfloat16)
            tail = jnp.dot(high, later, preferred_element_type=jnp.float32) + jnp.dot(
                low, later, preferred_element_type=jnp.float32
            )
            weight = jnp.where(live, jnp.exp(jnp.minimum(z, 0.0) - soft + tail + carried[h]), 0.0)
            totals[h] += jnp.dot(weight.astype(jnp.bfloat16), v, preferred_element_type=jnp.float32)
            carried[h] += tail[:, :1] + keep[:, :1]
    out[...] = jnp.concatenate(totals, axis=1).astype(jnp.bfloat16)


def attention(queries, blocks, offsets):
    rows, width = queries.shape
    heads = offsets.shape[0]
    vmem = pl.BlockSpec(memory_space=pltpu.VMEM)

    def body(*refs):
        attention_kernel(heads, width // heads, rows, *refs)

    return pl.pallas_call(
        body,
        out_shape=jax.ShapeDtypeStruct((rows, width), jnp.bfloat16),
        in_specs=[pl.BlockSpec(memory_space=pltpu.SMEM)] + [vmem] * (1 + len(blocks)),
        out_specs=vmem,
        compiler_params=pltpu.CompilerParams(vmem_limit_bytes=12 << 20),
        name="attention",
    )(offsets, queries, *blocks)


def ffn_kernel(cuts, ahead, x, weights, out, gate_up, down, sems):
    units = down.shape[1]
    half = down.shape[0] // 2

    def copy(source, target, sem):
        return pltpu.make_async_copy(source, target, sem)

    stages = []
    for i, (a, b) in enumerate(cuts):
        n = (b - a) // 2
        stages.append(
            [
                copy(
                    weights.at[pl.ds(at, n), pl.ds(0, 2 * units)],
                    gate_up.at[pl.ds(at, n)],
                    sems.at[2 * i + j],
                )
                for j, at in enumerate((a, a + n))
            ]
        )
    for j in range(2):
        rows = pl.ds(j * half, half)
        stages.append(
            [copy(weights.at[rows, pl.ds(2 * units, units)], down.at[rows], sems.at[2 * len(cuts) + j])]
        )

    def start(i):
        for one in stages[i] if i < len(stages) else ():
            one.start()

    def wait(i):
        for one in stages[i]:
            one.wait()
        start(i + ahead)

    for i in range(ahead):
        start(i)
    acc = None
    for i, (a, b) in enumerate(cuts):
        wait(i)
        term = jnp.dot(x[:, a:b], gate_up[a:b, :], preferred_element_type=jnp.float32)
        acc = term if acc is None else acc + term
    gate, upper = acc[:, :units], acc[:, units:]
    hidden = (gate / (1.0 + jnp.exp(-gate)) * upper).astype(jnp.bfloat16)
    for j in range(2):
        wait(len(cuts) + j)
        rows = slice(j * half, (j + 1) * half)
        out[:, rows] = lax.dot_general(
            hidden, down[rows, :], (((1,), (1,)), ((), ())), preferred_element_type=jnp.float32
        ).astype(jnp.bfloat16)


def ffn(x, weights, units):
    width = weights.shape[0]
    marks = (0, 3 * width // 8, 11 * width // 16, width)
    cuts = tuple(zip(marks[:-1], marks[1:]))
    vmem = pl.BlockSpec(memory_space=pltpu.VMEM)

    def body(*refs):
        ffn_kernel(cuts, 4, *refs)

    return pl.pallas_call(
        body,
        out_shape=jax.ShapeDtypeStruct(x.shape, jnp.bfloat16),
        in_specs=[vmem, pl.BlockSpec(memory_space=pltpu.HBM)],
        out_specs=vmem,
        scratch_shapes=[
            pltpu.VMEM((width, 2 * units), jnp.bfloat16),
            pltpu.VMEM((width, units), jnp.bfloat16),
            pltpu.SemaphoreType.DMA((2 * len(cuts) + 2,)),
        ],
        compiler_params=pltpu.CompilerParams(vmem_limit_bytes=48 << 20),
        name="ffn",
    )(x, weights)


def on_device(
    resid,
    queries,
    keys,
    values,
    doc_ids,
    score_offset,
    out_weight,
    norm_gain,
    gate_weight,
    up_weight,
    down_weight,
):
    rows = queries.shape[0]
    units = gate_weight.shape[1]
    packed = jnp.concatenate([gate_weight, up_weight, down_weight.T], axis=1)
    weights = lax.all_gather(packed, "sp", axis=0, tiled=True)

    docs = jnp.pad(doc_ids.astype(jnp.bfloat16)[None], ((0, 7), (0, 2 * keys.shape[1] - rows)))
    own = jnp.concatenate([jnp.concatenate([keys, values], axis=1), docs], axis=0)
    blocks = {0: own}
    blocks[7] = shifted(own, 7)
    for back in range(1, 5):
        blocks[back] = shifted(blocks[back - 1], 1)
        if back < 3:
            blocks[7 - back] = shifted(blocks[8 - back], -1)
    attended = attention(queries, [blocks[b] for b in range(8)], score_offset)

    mixed_attn = summed_for_owner(
        jnp.dot(attended, out_weight, preferred_element_type=jnp.float32).astype(jnp.bfloat16)
    )
    stream = resid.astype(jnp.float32) + mixed_attn
    normed = (
        stream * lax.rsqrt(jnp.mean(stream * stream, axis=1, keepdims=True) + 1e-06) * norm_gain
    ).astype(jnp.bfloat16)
    span_rows = from_everyone(normed).reshape(rows, -1)
    feed = summed_for_owner(ffn(span_rows, weights, units))
    return (stream + feed).astype(jnp.bfloat16)


def solution(mesh):
    in_specs = (
        P(("sp", "tp"), None),
        P("sp", "tp"),
        P("sp", "tp"),
        P("sp", "tp"),
        P("sp"),
        P("tp"),
        P("tp", None),
        P(),
        P("sp", "tp"),
        P("sp", "tp"),
        P("tp", "sp"),
    )
    out_specs = P(("sp", "tp"), None)
    return jax.shard_map(
        on_device, mesh=mesh, in_specs=in_specs, out_specs=out_specs, check_vma=False
    )
```

```python
import jax
import jax.numpy as jnp
from jax import lax
from jax.experimental import pallas as pl
from jax.experimental.pallas import tpu as pltpu
from jax.sharding import PartitionSpec as P


def shifted(block, by):
    spans = lax.axis_size("sp")
    return lax.ppermute(block, "sp", [(i, (i + by) % spans) for i in range(spans)])


def summed_for_owner(partial):
    peers = lax.axis_size("tp")
    tiles = partial.reshape(peers, partial.shape[0] // peers, partial.shape[1])
    tiles = lax.all_to_all(tiles, "tp", 0, 0, tiled=True)
    return jnp.sum(tiles.astype(jnp.float32), axis=0)


def from_everyone(shard):
    copies = jnp.broadcast_to(shard, (lax.axis_size("tp"), *shard.shape))
    return lax.all_to_all(copies, "tp", split_axis=0, concat_axis=0, tiled=True)


def attention_kernel(heads, head_dim, rows, offsets, queries, *refs):
    blocks, out = refs[:-1], refs[-1]
    width = heads * head_dim
    own_docs = blocks[0][rows : rows + 1, :rows].astype(jnp.float32)
    q_docs = jnp.broadcast_to(own_docs, (rows, rows)).T
    q_docs = jnp.concatenate([q_docs, q_docs], axis=1)
    r = lax.broadcasted_iota(jnp.int32, (rows, 2 * rows), 0)
    c = lax.broadcasted_iota(jnp.int32, (rows, 2 * rows), 1)
    causal = c - rows < r
    j = lax.broadcasted_iota(jnp.int32, (2 * rows, 2 * rows), 0)
    s = lax.broadcasted_iota(jnp.int32, (2 * rows, 2 * rows), 1)
    later = (j > s).astype(jnp.float32).astype(jnp.bfloat16)
    totals = [jnp.zeros((rows, head_dim), jnp.float32) for _ in range(heads)]
    carried = [jnp.zeros((rows, 1), jnp.float32) for _ in range(heads)]
    scale = head_dim ** (-0.5)
    for pair in range(len(blocks) // 2):
        near, far = blocks[2 * pair], blocks[2 * pair + 1]
        k_docs = jnp.concatenate([far[rows : rows + 1, :rows], near[rows : rows + 1, :rows]], axis=1)
        live = k_docs.astype(jnp.float32) == q_docs
        if pair == 0:
            live = live & causal
        for h in range(heads):
            cols = slice(h * head_dim, (h + 1) * head_dim)
            v_cols = slice(width + h * head_dim, width + (h + 1) * head_dim)
            k = jnp.concatenate([far[:rows, cols], near[:rows, cols]], axis=0)
            v = jnp.concatenate([far[:rows, v_cols], near[:rows, v_cols]], axis=0)
            z = lax.dot_general(
                queries[:, cols], k, (((1,), (1,)), ((), ())), preferred_element_type=jnp.float32
            ) * scale + offsets[h]
            soft = jnp.log(1.0 + jnp.exp(-jnp.abs(z)))
            keep = jnp.where(live, jnp.minimum(-z, 0.0) - soft, 0.0)
            high = keep.astype(jnp.bfloat16)
            low = (keep - high.astype(jnp.float32)).astype(jnp.bfloat16)
            tail = jnp.dot(high, later, preferred_element_type=jnp.float32) + jnp.dot(
                low, later, preferred_element_type=jnp.float32
            )
            weight = jnp.where(live, jnp.exp(jnp.minimum(z, 0.0) - soft + tail + carried[h]), 0.0)
            totals[h] += jnp.dot(weight.astype(jnp.bfloat16), v, preferred_element_type=jnp.float32)
            carried[h] += tail[:, :1] + keep[:, :1]
    out[...] = jnp.concatenate(totals, axis=1).astype(jnp.bfloat16)


def attention(queries, blocks, offsets):
    rows, width = queries.shape
    heads = offsets.shape[0]
    vmem = pl.BlockSpec(memory_space=pltpu.VMEM)

    def body(*refs):
        attention_kernel(heads, width // heads, rows, *refs)

    return pl.pallas_call(
        body,
        out_shape=jax.ShapeDtypeStruct((rows, width), jnp.bfloat16),
        in_specs=[pl.BlockSpec(memory_space=pltpu.SMEM)] + [vmem] * (1 + len(blocks)),
        out_specs=vmem,
        compiler_params=pltpu.CompilerParams(vmem_limit_bytes=12 << 20),
        name="attention",
    )(offsets, queries, *blocks)


def ffn_kernel(cuts, ahead, x, weights, out, gate_up, down, sems):
    units = down.shape[1]
    half = down.shape[0] // 2

    def copy(source, target, sem):
        return pltpu.make_async_copy(source, target, sem)

    stages = []
    for i, (a, b) in enumerate(cuts):
        n = (b - a) // 2
        stages.append(
            [
                copy(
                    weights.at[pl.ds(at, n), pl.ds(0, 2 * units)],
                    gate_up.at[pl.ds(at, n)],
                    sems.at[2 * i + j],
                )
                for j, at in enumerate((a, a + n))
            ]
        )
    for j in range(2):
        rows = pl.ds(j * half, half)
        stages.append(
            [copy(weights.at[rows, pl.ds(2 * units, units)], down.at[rows], sems.at[2 * len(cuts) + j])]
        )

    def start(i):
        for one in stages[i] if i < len(stages) else ():
            one.start()

    def wait(i):
        for one in stages[i]:
            one.wait()
        start(i + ahead)

    for i in range(ahead):
        start(i)
    acc = None
    for i, (a, b) in enumerate(cuts):
        wait(i)
        term = jnp.dot(x[:, a:b], gate_up[a:b, :], preferred_element_type=jnp.float32)
        acc = term if acc is None else acc + term
    gate, upper = acc[:, :units], acc[:, units:]
    hidden = (gate / (1.0 + jnp.exp(-gate)) * upper).astype(jnp.bfloat16)
    for j in range(2):
        wait(len(cuts) + j)
        rows = slice(j * half, (j + 1) * half)
        out[:, rows] = lax.dot_general(
            hidden, down[rows, :], (((1,), (1,)), ((), ())), preferred_element_type=jnp.float32
        ).astype(jnp.bfloat16)


def ffn(x, weights, units):
    width = weights.shape[0]
    marks = (0, 3 * width // 8, 11 * width // 16, width)
    cuts = tuple(zip(marks[:-1], marks[1:]))
    vmem = pl.BlockSpec(memory_space=pltpu.VMEM)

    def body(*refs):
        ffn_kernel(cuts, 4, *refs)

    return pl.pallas_call(
        body,
        out_shape=jax.ShapeDtypeStruct(x.shape, jnp.bfloat16),
        in_specs=[vmem, pl.BlockSpec(memory_space=pltpu.HBM)],
        out_specs=vmem,
        scratch_shapes=[
            pltpu.VMEM((width, 2 * units), jnp.bfloat16),
            pltpu.VMEM((width, units), jnp.bfloat16),
            pltpu.SemaphoreType.DMA((2 * len(cuts) + 2,)),
        ],
        compiler_params=pltpu.CompilerParams(vmem_limit_bytes=48 << 20),
        name="ffn",
    )(x, weights)


def on_device(
    resid,
    queries,
    keys,
    values,
    doc_ids,
    score_offset,
    out_weight,
    norm_gain,
    gate_weight,
    up_weight,
    down_weight,
):
    rows = queries.shape[0]
    units = gate_weight.shape[1]
    packed = jnp.concatenate([gate_weight, up_weight, down_weight.T], axis=1)
    weights = lax.all_gather(packed, "sp", axis=0, tiled=True)

    docs = jnp.pad(doc_ids.astype(jnp.bfloat16)[None], ((0, 7), (0, 2 * keys.shape[1] - rows)))
    own = jnp.concatenate([jnp.concatenate([keys, values], axis=1), docs], axis=0)
    blocks = {0: own}
    blocks[7] = shifted(own, 7)
    for back in range(1, 4):
        blocks[back] = shifted(blocks[back - 1], 1)
        if back < 3:
            blocks[7 - back] = shifted(blocks[8 - back], -1)
    width = keys.shape[1]
    blocks[4] = jnp.concatenate(
        [shifted(blocks[3][:, :width], 1), shifted(blocks[5][:, width:], -1)], axis=1
    )
    attended = attention(queries, [blocks[b] for b in range(8)], score_offset)

    mixed_attn = summed_for_owner(
        jnp.dot(attended, out_weight, preferred_element_type=jnp.float32).astype(jnp.bfloat16)
    )
    stream = resid.astype(jnp.float32) + mixed_attn
    normed = (
        stream * lax.rsqrt(jnp.mean(stream * stream, axis=1, keepdims=True) + 1e-06) * norm_gain
    ).astype(jnp.bfloat16)
    span_rows = from_everyone(normed).reshape(rows, -1)
    feed = summed_for_owner(ffn(span_rows, weights, units))
    return (stream + feed).astype(jnp.bfloat16)


def solution(mesh):
    in_specs = (
        P(("sp", "tp"), None),
        P("sp", "tp"),
        P("sp", "tp"),
        P("sp", "tp"),
        P("sp"),
        P("tp"),
        P("tp", None),
        P(),
        P("sp", "tp"),
        P("sp", "tp"),
        P("tp", "sp"),
    )
    out_specs = P(("sp", "tp"), None)
    return jax.shard_map(
        on_device, mesh=mesh, in_specs=in_specs, out_specs=out_specs, check_vma=False
    )
```

```python
import jax
import jax.numpy as jnp
from jax import lax
from jax.experimental import pallas as pl
from jax.experimental.pallas import tpu as pltpu
from jax.sharding import PartitionSpec as P


def shifted(block, by):
    spans = lax.axis_size("sp")
    return lax.ppermute(block, "sp", [(i, (i + by) % spans) for i in range(spans)])


def summed_for_owner(partial):
    peers = lax.axis_size("tp")
    tiles = partial.reshape(peers, partial.shape[0] // peers, partial.shape[1])
    tiles = lax.all_to_all(tiles, "tp", 0, 0, tiled=True)
    return jnp.sum(tiles.astype(jnp.float32), axis=0)


def from_everyone(shard):
    copies = jnp.broadcast_to(shard, (lax.axis_size("tp"), *shard.shape))
    return lax.all_to_all(copies, "tp", split_axis=0, concat_axis=0, tiled=True)


def attention_kernel(heads, head_dim, rows, offsets, queries, *refs):
    blocks, out = refs[:-1], refs[-1]
    width = heads * head_dim
    own_docs = blocks[0][rows : rows + 1, :rows].astype(jnp.float32)
    q_docs = jnp.broadcast_to(own_docs, (rows, rows)).T
    q_docs = jnp.concatenate([q_docs, q_docs], axis=1)
    r = lax.broadcasted_iota(jnp.int32, (rows, 2 * rows), 0)
    c = lax.broadcasted_iota(jnp.int32, (rows, 2 * rows), 1)
    causal = c - rows < r
    j = lax.broadcasted_iota(jnp.int32, (2 * rows, 2 * rows), 0)
    s = lax.broadcasted_iota(jnp.int32, (2 * rows, 2 * rows), 1)
    later = (j > s).astype(jnp.float32).astype(jnp.bfloat16)
    totals = [jnp.zeros((rows, head_dim), jnp.float32) for _ in range(heads)]
    carried = [jnp.zeros((rows, 1), jnp.float32) for _ in range(heads)]
    scale = head_dim ** (-0.5)
    for pair in range(len(blocks) // 2):
        near, far = blocks[2 * pair], blocks[2 * pair + 1]
        k_docs = jnp.concatenate([far[rows : rows + 1, :rows], near[rows : rows + 1, :rows]], axis=1)
        live = k_docs.astype(jnp.float32) == q_docs
        if pair == 0:
            live = live & causal
        for h in range(heads):
            cols = slice(h * head_dim, (h + 1) * head_dim)
            v_cols = slice(width + h * head_dim, width + (h + 1) * head_dim)
            k = jnp.concatenate([far[:rows, cols], near[:rows, cols]], axis=0)
            v = jnp.concatenate([far[:rows, v_cols], near[:rows, v_cols]], axis=0)
            z = lax.dot_general(
                queries[:, cols], k, (((1,), (1,)), ((), ())), preferred_element_type=jnp.float32
            ) * scale + offsets[h]
            soft = jnp.log(1.0 + jnp.exp(-jnp.abs(z)))
            keep = jnp.where(live, jnp.minimum(-z, 0.0) - soft, 0.0)
            high = keep.astype(jnp.bfloat16)
            low = (keep - high.astype(jnp.float32)).astype(jnp.bfloat16)
            tail = jnp.dot(high, later, preferred_element_type=jnp.float32) + jnp.dot(
                low, later, preferred_element_type=jnp.float32
            )
            weight = jnp.where(live, jnp.exp(jnp.minimum(z, 0.0) - soft + tail + carried[h]), 0.0)
            totals[h] += jnp.dot(weight.astype(jnp.bfloat16), v, preferred_element_type=jnp.float32)
            carried[h] += tail[:, :1] + keep[:, :1]
    out[...] = jnp.concatenate(totals, axis=1).astype(jnp.bfloat16)


def attention(queries, blocks, offsets):
    rows, width = queries.shape
    heads = offsets.shape[0]
    vmem = pl.BlockSpec(memory_space=pltpu.VMEM)

    def body(*refs):
        attention_kernel(heads, width // heads, rows, *refs)

    return pl.pallas_call(
        body,
        out_shape=jax.ShapeDtypeStruct((rows, width), jnp.bfloat16),
        in_specs=[pl.BlockSpec(memory_space=pltpu.SMEM)] + [vmem] * (1 + len(blocks)),
        out_specs=vmem,
        compiler_params=pltpu.CompilerParams(vmem_limit_bytes=12 << 20),
        name="attention",
    )(offsets, queries, *blocks)


def ffn_kernel(cuts, ahead, x, weights, out, gate_up, down, sems):
    units = down.shape[1]
    half = down.shape[0] // 2

    def copy(source, target, sem):
        return pltpu.make_async_copy(source, target, sem)

    stages = []
    for i, (a, b) in enumerate(cuts):
        n = (b - a) // 2
        stages.append(
            [
                copy(
                    weights.at[pl.ds(at, n), pl.ds(0, 2 * units)],
                    gate_up.at[pl.ds(at, n)],
                    sems.at[2 * i + j],
                )
                for j, at in enumerate((a, a + n))
            ]
        )
    for j in range(2):
        rows = pl.ds(j * half, half)
        stages.append(
            [copy(weights.at[rows, pl.ds(2 * units, units)], down.at[rows], sems.at[2 * len(cuts) + j])]
        )

    def start(i):
        for one in stages[i] if i < len(stages) else ():
            one.start()

    def wait(i):
        for one in stages[i]:
            one.wait()
        start(i + ahead)

    for i in range(ahead):
        start(i)
    acc = None
    for i, (a, b) in enumerate(cuts):
        wait(i)
        term = jnp.dot(x[:, a:b], gate_up[a:b, :], preferred_element_type=jnp.float32)
        acc = term if acc is None else acc + term
    gate, upper = acc[:, :units], acc[:, units:]
    hidden = (gate / (1.0 + jnp.exp(-gate)) * upper).astype(jnp.bfloat16)
    for j in range(2):
        wait(len(cuts) + j)
        rows = slice(j * half, (j + 1) * half)
        out[:, rows] = lax.dot_general(
            hidden, down[rows, :], (((1,), (1,)), ((), ())), preferred_element_type=jnp.float32
        ).astype(jnp.bfloat16)


def ffn(x, weights, units):
    width = weights.shape[0]
    marks = (0, 3 * width // 8, 11 * width // 16, width)
    cuts = tuple(zip(marks[:-1], marks[1:]))
    vmem = pl.BlockSpec(memory_space=pltpu.VMEM)

    def body(*refs):
        ffn_kernel(cuts, 4, *refs)

    return pl.pallas_call(
        body,
        out_shape=jax.ShapeDtypeStruct(x.shape, jnp.bfloat16),
        in_specs=[vmem, pl.BlockSpec(memory_space=pltpu.HBM)],
        out_specs=vmem,
        scratch_shapes=[
            pltpu.VMEM((width, 2 * units), jnp.bfloat16),
            pltpu.VMEM((width, units), jnp.bfloat16),
            pltpu.SemaphoreType.DMA((2 * len(cuts) + 2,)),
        ],
        compiler_params=pltpu.CompilerParams(vmem_limit_bytes=48 << 20),
        name="ffn",
    )(x, weights)


def on_device(
    resid,
    queries,
    keys,
    values,
    doc_ids,
    score_offset,
    out_weight,
    norm_gain,
    gate_weight,
    up_weight,
    down_weight,
):
    rows = queries.shape[0]
    units = gate_weight.shape[1]
    packed = jnp.concatenate([gate_weight, up_weight, down_weight.T], axis=1)
    weights = lax.all_gather(packed, "sp", axis=0, tiled=True)

    docs = jnp.pad(doc_ids.astype(jnp.bfloat16)[None], ((0, 7), (0, 2 * keys.shape[1] - rows)))
    own = jnp.concatenate([jnp.concatenate([keys, values], axis=1), docs], axis=0)
    blocks = {0: own}
    blocks[7] = shifted(own, 7)
    for back in range(1, 4):
        blocks[back] = shifted(blocks[back - 1], 1)
        if back < 4:
            blocks[7 - back] = shifted(blocks[8 - back], -1)
    attended = attention(queries, [blocks[b] for b in range(8)], score_offset)

    mixed_attn = summed_for_owner(
        jnp.dot(attended, out_weight, preferred_element_type=jnp.float32).astype(jnp.bfloat16)
    )
    stream = resid.astype(jnp.float32) + mixed_attn
    normed = (
        stream * lax.rsqrt(jnp.mean(stream * stream, axis=1, keepdims=True) + 1e-06) * norm_gain
    ).astype(jnp.bfloat16)
    span_rows = from_everyone(normed).reshape(rows, -1)
    feed = summed_for_owner(ffn(span_rows, weights, units))
    return (stream + feed).astype(jnp.bfloat16)


def solution(mesh):
    in_specs = (
        P(("sp", "tp"), None),
        P("sp", "tp"),
        P("sp", "tp"),
        P("sp", "tp"),
        P("sp"),
        P("tp"),
        P("tp", None),
        P(),
        P("sp", "tp"),
        P("sp", "tp"),
        P("tp", "sp"),
    )
    out_specs = P(("sp", "tp"), None)
    return jax.shard_map(
        on_device, mesh=mesh, in_specs=in_specs, out_specs=out_specs, check_vma=False
    )
```
